256 devices in a mesh: ep: 64 (over z, x, core), tp: 4 (over y).
Axes of the slice: x: 4, y: 4, z: 8, core: 2. Of those that a mesh axis runs over, the one named last changes fastest.
Arguments:
- tokens: bfloat16 [512, 2048], P('ep'), may hold values from -6 to 6
- lengths: int32 [512], P('ep'), may hold values from 1 to 1024, as said below
- cache_keys: bfloat16 [512, 4, 1024, 128], P('ep', 'tp'), may hold values from -120 to 120
- cache_values: bfloat16 [512, 4, 1024, 128], P('ep', 'tp'), may hold values from -6 to 6
- w_query: bfloat16 [2048, 2048], P('ep', 'tp'), may hold values from -0.21875 to 0.21875
- w_key: bfloat16 [2048, 512], P('ep', 'tp'), may hold values from -0.125 to 0.125
- w_value: bfloat16 [2048, 512], P('ep', 'tp'), may hold values from -0.125 to 0.125
- mix_weight: float32 [16], P('tp'), may hold values from 0.3 to 0.8
- head_gain: float32 [128], replicated, may hold values from 0.1 to 1.9
- w_out: bfloat16 [2048, 2048], P('tp', 'ep'), may hold values from -0.125 to 0.125
- first_gain: float32 [2048], replicated, may hold values from 0.1 to 1.9
- routing: int32 [512, 2], P('ep'), may hold values from 0 to 15, all different within a row; in each aligned block of 8 rows (0 to 7, 8 to 15, ...) at most 2 rows name the same one
- route_weights: float32 [512, 2], P('ep'), may hold values from 0.1 to 0.9
- expert_gate: bfloat16 [64, 2048, 1408], P('ep', None, 'tp'), may hold values from -0.125 to 0.125
- expert_up: bfloat16 [64, 2048, 1408], P('ep', None, 'tp'), may hold values from -0.125 to 0.125
- expert_down: bfloat16 [64, 1408, 2048], P('ep', None, 'tp'), may hold values from -0.078125 to 0.078125
- dense_gate: bfloat16 [2048, 4096], P('tp', 'ep'), may hold values from -0.125 to 0.125
- dense_up: bfloat16 [2048, 4096], P('tp', 'ep'), may hold values from -0.125 to 0.125
- dense_down: bfloat16 [4096, 2048], P('ep', 'tp'), may hold values from -0.09375 to 0.09375
- switch_vector: float32 [2048], replicated, may hold values from -0.25 to 0.25
- final_gain: float32 [2048], P('tp'), may hold values from 0.1 to 1.9
Outputs:
- mixed: bfloat16 [512, 2048], P('ep', 'tp')
The draws below stay inside these ranges and needn't reach their ends.
Inputs may be any that keep to these rules, and one draw needn't show every extreme that they name: `lengths`: every sequence has at least one cached position; some sequence has exactly 1024. `routing`: each row names 2 different experts; among the rows of one index of ep no expert is named more than 2 times, a bound that some block reaches.
All inputs are finite; a program needn't handle non-finite values.
Results may differ from the reference program's by a relative error of at most 0.015.
The reference program's roundings to bfloat16 on the way count: a program that leaves them out, or rounds other values in their place, can miss the bound.
Values may be sent and summed in bfloat16 or wider, within the bound.
A program may use at most 64 MiB of HBM per device.

```python
import math
import jax
import jax.numpy as jnp
import numpy as np
from jax import lax

D = 2048
H = 16
KVH = 4
QK = 128
HEAD = 64
FF_E = 5632
FF_D = 4096
SPAN = 4
TOP = 2
SEQ_GRP = 8
LEN = 1024
BATCH = 512
EXPERTS = 16
CAP = 2
N_EP = 64
N_TP = 4


def draw_lengths(key, part):
    first = jax.random.randint(jax.random.fold_in(key, 11), (BATCH,), 1, LEN + 1)
    second = jax.random.randint(jax.random.fold_in(key, 12), (BATCH,), 1, LEN + 1)
    heavy = jax.random.randint(jax.random.fold_in(key, 13), (BATCH // SEQ_GRP, 1), 0, 4) == 0
    heavy = jnp.broadcast_to(heavy, (BATCH // SEQ_GRP, SEQ_GRP)).reshape(BATCH)
    lengths = jnp.where(heavy, jnp.maximum(first, second), jnp.minimum(first, second))
    filled = jax.random.randint(jax.random.fold_in(key, 14), (), 0, BATCH)
    return lengths.at[filled].set(LEN).astype(jnp.int32)


def draw_cache_keys(key, part):
    shape = (BATCH, KVH, LEN, QK)
    base = jnp.clip(jax.random.normal(jax.random.fold_in(key, 24), shape, jnp.float32), -6.0, 6.0)
    return base.astype(jnp.bfloat16)


def block_levels(rng, extent, cuts, low, high):
    loudness = 1.0
    for position, blocks in cuts:
        draws = jax.random.uniform(jax.random.fold_in(jax.random.fold_in(rng, 6), position), (blocks,), jnp.float32, low / len(cuts), high / len(cuts))
        loudness = loudness * jnp.repeat(jnp.exp(draws), extent[position] // blocks).reshape((-1,) + (1,) * (len(extent) - 1 - position))
    return loudness


def routed_block(own_key, own, number, rows, amount, top, reach, lean):
    order = jax.random.permutation(own_key, amount)
    packed, common = load_shares(amount, rows * top, reach, lean, True), load_shares(amount, rows * top, reach, lean, False)
    places = jnp.arange(amount)

    def named(sizes, rotation):
        used = int((sizes > 0).sum())
        fixed = max(1, used // 4)
        shifted = fixed + (places - fixed + rotation * (used - fixed)) % max(1, amount - fixed)
        return jnp.zeros((amount,), jnp.int32).at[order[jnp.where(places < fixed, places, shifted)]].set(jnp.asarray(sizes, jnp.int32))

    sizes = jnp.where(number % 4 == 0, named(packed, number // 4), named(common, number - number // 4 - 1))
    mixed = jax.random.permutation(jax.random.fold_in(own, 3), amount)
    giver, receiver = mixed[0:amount // 2 * 2:2], mixed[1:amount // 2 * 2:2]
    margin = jnp.minimum(sizes[giver] - 1, reach - sizes[receiver]) // 2
    margin = jnp.where((giver == order[0]) | (receiver == order[0]) | (sizes[receiver] == 0), 0, jnp.maximum(margin, 0))
    shifted = jax.random.randint(jax.random.fold_in(own, 4), (amount // 2,), 0, 1 << 20) % (margin + 1)
    sizes = sizes.at[giver].add(-shifted).at[receiver].add(shifted)
    items = jnp.searchsorted(jnp.cumsum(sizes), jnp.arange(rows * top), side="right").astype(jnp.int32)
    table = items.reshape(top, rows).T
    table = table[jax.random.permutation(jax.random.fold_in(own, 1), rows)]
    rotation = jax.random.randint(jax.random.fold_in(own, 2), (rows, 1), 0, top)
    return jnp.take_along_axis(table, (jnp.arange(top)[None, :] + rotation) % top, axis=1)


def load_shares(count, total, most, skew, full):
    weights = [(1 << 20) // math.isqrt(rank ** skew) + 1 for rank in range(1, count + 1)]
    largest = most if full else min(most, max(-(-total // count), total * weights[0] // sum(weights)))
    least = 1 if total - largest >= count - 1 else 0
    given, spare = [largest] + [least] * (count - 1), total - largest - least * (count - 1)
    while spare > 0:
        free = [i for i in range(1, count) if given[i] < largest] or [i for i in range(1, count) if given[i] < most]
        whole, budget = sum([weights[i] for i in free]), spare
        for i in free:
            more = min(most - given[i], max(1, budget * weights[i] // whole), spare)
            given[i] = given[i] + more
            spare = spare - more
    return np.array(given)


def normal_values(rng, shape, deviation, bound, pieces=(), kind=jnp.bfloat16):
    values = jax.random.normal(rng, shape, jnp.float32) * deviation
    if len(pieces) > 0:
        values = block_levels(rng, shape, pieces, -0.22, 0.18) * values
    return jnp.clip(values, min=-bound, max=bound).astype(kind)


def setup_inputs(seed: int = 0) -> dict:
    arg_keys = jax.random.split(jax.random.key(seed), 22)
    tokens = normal_values(arg_keys[0], (BATCH, D), 1.0, 6.0, ((0, 64),))
    lengths = draw_lengths(jax.random.fold_in(arg_keys[21], 71), 0)
    cache_keys = draw_cache_keys(jax.random.fold_in(arg_keys[21], 71), 0)
    cache_values = normal_values(arg_keys[3], (BATCH, KVH, LEN, QK), 1.0, 6.0, ((0, 64), (1, 4)))
    w_query = normal_values(arg_keys[4], (D, H * QK), (D // 3) ** -0.5, 0.21875, ((0, 64), (1, 4)))
    w_key = normal_values(arg_keys[5], (D, KVH * QK), D ** -0.5, 0.125, ((0, 64), (1, 4)))
    w_value = normal_values(arg_keys[6], (D, KVH * QK), D ** -0.5, 0.125, ((0, 64), (1, 4)))
    mix_weight = jnp.clip(0.3 + 0.5 * jax.random.uniform(arg_keys[7], (H,), jnp.float32) ** block_levels(arg_keys[7], (H,), ((0, 4),), -0.2, 0.2), 0.3, 0.8)
    head_gain = jnp.clip(1.0 + 0.18 * jax.random.normal(arg_keys[8], (QK,), jnp.float32), 0.1, 1.9)
    w_out = normal_values(arg_keys[9], (H * QK, D), (H * QK) ** -0.5, 0.125, ((0, 4), (1, 64)))
    first_gain = jnp.clip(1.0 + 0.18 * jax.random.normal(arg_keys[10], (D,), jnp.float32), 0.1, 1.9)
    routing_keys = jax.random.split(jax.random.fold_in(arg_keys[11], 1), BATCH // SEQ_GRP)
    routing_turns = jax.random.permutation(jax.random.fold_in(arg_keys[11], 3), BATCH // SEQ_GRP)
    routing = jax.vmap(lambda own, number: routed_block(jax.random.fold_in(arg_keys[11], 2), own, number, SEQ_GRP, EXPERTS, TOP, CAP, 2))(routing_keys, routing_turns).reshape((BATCH, TOP))
    route_weights = jnp.clip(0.1 + 0.79999997 * jax.random.uniform(arg_keys[12], (BATCH, TOP), jnp.float32) ** block_levels(arg_keys[12], (BATCH, TOP), ((0, 64),), -0.2, 0.2), 0.1, 0.9)
    expert_gate = normal_values(arg_keys[13], (EXPERTS * SPAN, D, FF_E // SPAN), D ** -0.5, 0.125, ((0, 64), (2, 4)))
    expert_up = normal_values(arg_keys[14], (EXPERTS * SPAN, D, FF_E // SPAN), D ** -0.5, 0.125, ((0, 64), (2, 4)))
    expert_down = normal_values(arg_keys[15], (EXPERTS * SPAN, FF_E // SPAN, D), FF_E ** -0.5, 0.078125, ((0, 64), (2, 4)))
    dense_gate = normal_values(arg_keys[16], (D, FF_D), D ** -0.5, 0.125, ((0, 4), (1, 64)))
    dense_up = normal_values(arg_keys[17], (D, FF_D), D ** -0.5, 0.125, ((0, 4), (1, 64)))
    dense_down = normal_values(arg_keys[18], (FF_D, D), FF_D ** -0.5, 0.09375, ((0, 64), (1, 4)))
    switch_vector = normal_values(arg_keys[19], (D,), (D // 4) ** -0.5, 0.25, (), jnp.float32)
    final_gain = jnp.clip(1.0 + 0.18 * jax.random.normal(arg_keys[20], (D,), jnp.float32), 0.1, 1.9)
    return {"tokens": tokens, "lengths": lengths, "cache_keys": cache_keys, "cache_values": cache_values, "w_query": w_query, "w_key": w_key, "w_value": w_value, "mix_weight": mix_weight, "head_gain": head_gain, "w_out": w_out, "first_gain": first_gain, "routing": routing, "route_weights": route_weights, "expert_gate": expert_gate, "expert_up": expert_up, "expert_down": expert_down, "dense_gate": dense_gate, "dense_up": dense_up, "dense_down": dense_down, "switch_vector": switch_vector, "final_gain": final_gain}


EPS = 1e-05

def layer_norm(values, gain):
    mean = lax.optimization_barrier(jnp.mean(values, axis=-1, keepdims=True))
    spread = lax.optimization_barrier(jnp.mean(jnp.square(values - mean), axis=-1, keepdims=True))
    return (values - mean) * lax.rsqrt(spread + EPS) * gain

def attend_block(query, key_new, value_new, keys, values, lengths, mix_weight, head_gain):
    f32 = jnp.float32
    seqs = query.shape[0]
    rep = H // KVH
    query = query.reshape(seqs, KVH, rep, 2, HEAD).astype(f32)
    key_new = key_new.reshape(seqs, KVH, 2, HEAD).astype(f32)
    value_new = value_new.reshape(seqs, KVH, QK).astype(f32)
    keys = keys.reshape(seqs, KVH, LEN, 2, HEAD).astype(f32)
    scale = HEAD ** (-0.5)
    cached = jnp.einsum('bgrmd,bglmd->bmgrl', query, keys) * scale
    own = jnp.einsum('bgrmd,bgmd->bmgr', query, key_new) * scale
    valid = (jnp.arange(LEN, dtype=jnp.int32)[None, :] < lengths[:, None])[:, None, None, None, :]
    cached = jnp.where(valid, cached, -jnp.inf)
    top = jnp.maximum(lax.optimization_barrier(jnp.max(cached, axis=-1)), own)
    cached_exp = jnp.exp(cached - top[..., None])
    own_exp = jnp.exp(own - top)
    total = lax.optimization_barrier(jnp.sum(cached_exp, axis=-1)) + own_exp
    lam = mix_weight.reshape(KVH, rep)
    mix_cached = (cached_exp[:, 0] / total[:, 0][..., None] - lam[None, :, :, None] * cached_exp[:, 1] / total[:, 1][..., None]).astype(jnp.bfloat16)
    mix_own = (own_exp[:, 0] / total[:, 0] - lam[None] * own_exp[:, 1] / total[:, 1]).astype(jnp.bfloat16)
    head_out = jnp.einsum('bgrl,bgld->bgrd', mix_cached.astype(f32), values.astype(f32))
    head_out = head_out + mix_own.astype(f32)[..., None] * value_new[:, :, None, :]
    square = lax.optimization_barrier(jnp.mean(jnp.square(head_out), axis=-1, keepdims=True))
    normed = head_out * lax.rsqrt(square + EPS) * head_gain
    return normed.astype(jnp.bfloat16).reshape(seqs, H * QK)

def reference(tokens, lengths, cache_keys, cache_values, w_query, w_key, w_value, mix_weight, head_gain, w_out, first_gain, routing, route_weights, expert_gate, expert_up, expert_down, dense_gate, dense_up, dense_down, switch_vector, final_gain):
    f32 = jnp.float32
    bf16 = jnp.bfloat16
    batch = tokens.shape[0]
    query = jnp.dot(tokens, w_query, preferred_element_type=f32).astype(bf16)
    key_new = jnp.dot(tokens, w_key, preferred_element_type=f32).astype(bf16)
    value_new = jnp.dot(tokens, w_value, preferred_element_type=f32).astype(bf16)
    blocks = batch // SEQ_GRP

    def one_block(items):
        return attend_block(items[0], items[1], items[2], items[3], items[4], items[5], mix_weight, head_gain)
    normed = lax.map(one_block, (query.reshape(blocks, SEQ_GRP, -1), key_new.reshape(blocks, SEQ_GRP, -1), value_new.reshape(blocks, SEQ_GRP, -1), cache_keys.reshape((blocks, SEQ_GRP) + cache_keys.shape[1:]), cache_values.reshape((blocks, SEQ_GRP) + cache_values.shape[1:]), lengths.reshape(blocks, SEQ_GRP)))
    normed = normed.reshape(batch, H * QK)
    group_cols = H * QK // N_TP
    attention = jnp.zeros((batch, D), f32)
    for group in range(N_TP):
        part = jnp.dot(normed[:, group * group_cols:(group + 1) * group_cols], w_out[group * group_cols:(group + 1) * group_cols], preferred_element_type=f32).astype(bf16)
        attention = attention + lax.optimization_barrier(part).astype(f32)
    hidden_state = layer_norm(tokens.astype(f32) + attention, first_gain).astype(bf16)
    flat_route = routing.reshape(-1)
    flat_weight = route_weights.reshape(-1)
    flat_token = (jnp.arange(batch * TOP, dtype=jnp.int32) // TOP).astype(jnp.int32)
    most = N_EP * CAP

    def one_slice(total, index):
        expert = index // SPAN
        hit = flat_route == expert
        picked = jnp.nonzero(hit, size=most, fill_value=0)[0].astype(jnp.int32)
        live = jnp.arange(most, dtype=jnp.int32) < jnp.sum(hit.astype(jnp.int32))
        rows = hidden_state[flat_token[picked]]
        gate = jnp.dot(rows, expert_gate[index], preferred_element_type=f32)
        lift = jnp.dot(rows, expert_up[index], preferred_element_type=f32)
        block_hidden = (jax.nn.silu(gate) * lift).astype(bf16)
        block_out = jnp.dot(block_hidden, expert_down[index], preferred_element_type=f32).astype(bf16)
        block_out = lax.optimization_barrier(block_out).astype(f32)
        weight = jnp.where(live, flat_weight[picked], jnp.zeros((), f32))
        total = total.at[flat_token[picked]].add(weight[:, None] * block_out)
        return (total, None)
    routed = lax.scan(one_slice, jnp.zeros((batch, D), f32), jnp.arange(N_EP, dtype=jnp.int32))[0]
    pre_gate = jnp.dot(hidden_state, dense_gate, preferred_element_type=f32)
    pre_up = jnp.dot(hidden_state, dense_up, preferred_element_type=f32)
    dense_hidden = (jax.nn.silu(pre_gate) * pre_up).astype(bf16)
    dense_out = jnp.dot(dense_hidden, dense_down, preferred_element_type=f32).astype(bf16)
    switch = jax.nn.sigmoid(lax.optimization_barrier(jnp.sum(hidden_state.astype(f32) * switch_vector, axis=-1)))
    combined = hidden_state.astype(f32) + routed + switch[:, None] * dense_out.astype(f32)
    return layer_norm(combined, final_gain).astype(bf16)
```

```python
from types import SimpleNamespace

import jax
import jax.numpy as jnp
from jax import lax
from jax.experimental import pallas as pl
from jax.experimental.pallas import tpu as pltpu
from jax.sharding import PartitionSpec as P

QK = 128
HEAD = 64
SPAN = 4
TOP = 2


EPS = 1e-05


NZ, NQ, NT = 8, 8, 4
MESH_ID = pl.DeviceIdType.MESH
F32 = jnp.float32
BF16 = jnp.bfloat16
NT_DIMS = (((1,), (1,)), ((), ()))


def dot(a, b):
    return jnp.dot(a, b, preferred_element_type=F32)


def dot_nt(a, b):
    return lax.dot_general(a, b, NT_DIMS, preferred_element_type=F32)


def eye(n):
    r = lax.broadcasted_iota(jnp.int32, (n, n), 0)
    c = lax.broadcasted_iota(jnp.int32, (n, n), 1)
    return jnp.where(r == c, 1.0, 0.0).astype(BF16)


def stacked(ref, n):
    return jnp.concatenate([ref[i].astype(F32) for i in range(n)], axis=0).astype(BF16)


A_SCRATCH = dict(
    tok_v=pltpu.VMEM((8, 2048), BF16),
    tokg=pltpu.VMEM((NZ, 8, 256), BF16),
    wg=pltpu.VMEM((256, 768), BF16),
    wo_raw=pltpu.VMEM((512, 32), BF16),
    wog=pltpu.VMEM((256, 512), BF16),
    kbuf=pltpu.VMEM((8, 1024, 128), BF16),
    vbuf=pltpu.VMEM((8, 1024, 128), BF16),
    fg_v=pltpu.VMEM((1, 2048), F32),
    hg_v=pltpu.VMEM((1, 128), F32),
    pbuf=pltpu.VMEM((NZ, 8, 768), F32),
    precv=pltpu.VMEM((NZ, 8, 768), F32),
    qv=pltpu.VMEM((8, 768), F32),
    qs=pltpu.VMEM((8, 8, 128), F32),
    nv=pltpu.VMEM((8, 512), F32),
    ng=pltpu.VMEM((NQ, 8, 512), BF16),
    gbuf=pltpu.VMEM((NQ, 8, 256), BF16),
    attr=pltpu.VMEM((NT, NQ, 8, 256), BF16),
    lsem=pltpu.SemaphoreType.DMA((10,)),
    s_wg=pltpu.SemaphoreType.DMA((NQ,)),
    r_wg=pltpu.SemaphoreType.DMA((NQ,)),
    s_tok=pltpu.SemaphoreType.DMA((NZ,)),
    r_tok=pltpu.SemaphoreType.DMA((NZ,)),
    s_wo=pltpu.SemaphoreType.DMA((NZ,)),
    r_wo=pltpu.SemaphoreType.DMA((NZ,)),
    s_p=pltpu.SemaphoreType.DMA((NZ,)),
    r_p=pltpu.SemaphoreType.DMA((NZ,)),
    s_n=pltpu.SemaphoreType.DMA((NQ,)),
    r_n=pltpu.SemaphoreType.DMA((NQ,)),
    s_a=pltpu.SemaphoreType.DMA((NT * NQ,)),
    r_a=pltpu.SemaphoreType.DMA((NT * NQ,)),
)


def remote(src, dst, send, recv, ep, tp):
    return pltpu.make_async_remote_copy(
        src_ref=src, dst_ref=dst, send_sem=send, recv_sem=recv,
        device_id=(ep, tp), device_id_type=MESH_ID,
    )


def where_am_i():
    ep, tp = lax.axis_index("ep"), lax.axis_index("tp")
    return ep // NQ, lax.rem(ep, NQ), tp


def attention_kernel(
    lengths, mixw, tokens, keys, values, wq, wk, wv, wout, hgain, fgain, out, *scratch
):
    s = SimpleNamespace(**dict(zip(A_SCRATCH, scratch)))
    z, q, y = where_am_i()
    me = z * NQ + q

    qrow = pl.multiple_of(q * 32, 32)
    zrow = pl.multiple_of(z * 32, 32)
    first = [
        pltpu.make_async_copy(tokens, s.tok_v, s.lsem.at[0]),
        pltpu.make_async_copy(wq, s.wg.at[pl.ds(qrow, 32), pl.ds(0, 512)], s.lsem.at[1]),
        pltpu.make_async_copy(wk, s.wg.at[pl.ds(qrow, 32), pl.ds(512, 128)], s.lsem.at[2]),
        pltpu.make_async_copy(wv, s.wg.at[pl.ds(qrow, 32), pl.ds(640, 128)], s.lsem.at[3]),
        pltpu.make_async_copy(wout, s.wo_raw, s.lsem.at[4]),
    ]
    later = [
        pltpu.make_async_copy(keys, s.kbuf, s.lsem.at[5]),
        pltpu.make_async_copy(values, s.vbuf, s.lsem.at[6]),
        pltpu.make_async_copy(fgain, s.fg_v, s.lsem.at[7]),
        pltpu.make_async_copy(hgain, s.hg_v, s.lsem.at[8]),
    ]
    for c in first:
        c.start()

    barrier = pltpu.get_barrier_semaphore()
    for d in range(1, NZ):
        pl.semaphore_signal(
            barrier, inc=1, device_id=(lax.rem(z + d, NZ) * NQ + q, y), device_id_type=MESH_ID
        )
    for dy in range(NT):
        for dq in range(NQ):
            if dy or dq:
                pl.semaphore_signal(
                    barrier, inc=1,
                    device_id=(z * NQ + lax.rem(q + dq, NQ), lax.rem(y + dy, NT)),
                    device_id_type=MESH_ID,
                )
    for c in later:
        c.start()
    first[4].wait()
    s.wog[pl.ds(zrow, 32), :] = dot_nt(eye(32), s.wo_raw[...]).astype(BF16)
    for c in first[:4]:
        c.wait()
    pl.semaphore_wait(barrier, NZ - 1 + NT * NQ - 1)

    wg_copies, tok_copies, wo_copies = [], [], []
    for d in range(1, NZ):
        zz = lax.rem(z + d, NZ)
        c = remote(
            s.tok_v.at[:, pl.ds(pl.multiple_of(zz * 256, 256), 256)], s.tokg.at[z],
            s.s_tok.at[d], s.r_tok.at[d], zz * NQ + q, y,
        )
        c.start()
        tok_copies.append(c)
    for d in range(1, NQ):
        mine = s.wg.at[pl.ds(qrow, 32), :]
        c = remote(mine, mine, s.s_wg.at[d], s.r_wg.at[d], z * NQ + lax.rem(q + d, NQ), y)
        c.start()
        wg_copies.append(c)
    for d in range(1, NZ):
        mine = s.wog.at[pl.ds(zrow, 32), :]
        c = remote(mine, mine, s.s_wo.at[d], s.r_wo.at[d], lax.rem(z + d, NZ) * NQ + q, y)
        c.start()
        wo_copies.append(c)
    s.tokg[z] = s.tok_v[:, pl.ds(pl.multiple_of(z * 256, 256), 256)]

    for c in tok_copies + wg_copies:
        c.wait_recv()
    part = dot(stacked(s.tokg, NZ), s.wg[...])
    for i in range(NZ):
        s.pbuf[i] = part[i * 8:(i + 1) * 8]
    p_copies = []
    for d in range(1, NZ):
        zz = lax.rem(z + d, NZ)
        c = remote(s.pbuf.at[zz], s.precv.at[z], s.s_p.at[d], s.r_p.at[d], zz * NQ + q, y)
        c.start()
        p_copies.append(c)
    s.precv[z] = s.pbuf[z]
    for c in p_copies:
        c.wait_recv()
    total = s.precv[0]
    for i in range(1, NZ):
        total = total + s.precv[i]
    s.qv[...] = total.astype(BF16).astype(F32)
    for b in range(8):
        for r in range(4):
            row = s.qv[b:b + 1, r * 128:(r + 1) * 128]
            s.qs[b, r:r + 1, :] = row
            s.qs[b, r + 4:r + 5, :] = row

    for c in later:
        c.wait()
    sub = lax.broadcasted_iota(jnp.int32, (8, 128), 0)
    lane = lax.broadcasted_iota(jnp.int32, (8, 128), 1)
    half = (sub >= 4) == (lane >= 64)
    col = lax.broadcasted_iota(jnp.int32, (8, 1024), 1)
    rows1 = lax.broadcasted_iota(jnp.int32, (8, 1), 0)
    lam = jnp.zeros((8, 1), F32)
    for r in range(4):
        lam = jnp.where(rows1 == r + 4, mixw[r], lam)
    weight = jnp.where(rows1 < 4, 1.0, -lam)
    for b in range(8):
        q8 = jnp.where(half, s.qs[b], 0.0)
        knew = s.qv[b:b + 1, 512:640]
        vnew = s.qv[b:b + 1, 640:768]
        sc = dot_nt(q8.astype(BF16), s.kbuf[b]) * 0.125
        own = jnp.sum(q8 * knew, axis=1, keepdims=True) * 0.125
        sc = jnp.where(col < lengths[b], sc, -jnp.inf)
        top = jnp.maximum(jnp.max(sc, axis=1, keepdims=True), own)
        e = jnp.exp(sc - top)
        eo = jnp.exp(own - top)
        scale = weight / (jnp.sum(e, axis=1, keepdims=True) + eo)
        t = e * scale
        mix = (t + pltpu.roll(t, 4, 0)).astype(BF16)
        to = jnp.broadcast_to(eo * scale, (8, 128))
        mix_own = (to + pltpu.roll(to, 4, 0)).astype(BF16).astype(F32)
        ho = dot(mix, s.vbuf[b]) + mix_own * vnew
        square = jnp.mean(ho * ho, axis=1, keepdims=True)
        n8 = ho * lax.rsqrt(square + EPS) * s.hg_v[...]
        for r in range(4):
            s.nv[b:b + 1, r * 128:(r + 1) * 128] = n8[r:r + 1, :]
    s.ng[q] = s.nv[...].astype(BF16)
    n_copies = []
    for d in range(1, NQ):
        c = remote(
            s.ng.at[q], s.ng.at[q], s.s_n.at[d], s.r_n.at[d], z * NQ + lax.rem(q + d, NQ), y
        )
        c.start()
        n_copies.append(c)
    for c in wo_copies + n_copies:
        c.wait_recv()
    group = dot_nt(stacked(s.ng, NQ), s.wog[...])
    for i in range(NQ):
        s.gbuf[i] = group[i * 8:(i + 1) * 8].astype(BF16)
    a_copies = []
    for dy in range(NT):
        for dq in range(NQ):
            if dy or dq:
                qq = lax.rem(q + dq, NQ)
                c = remote(
                    s.gbuf.at[qq], s.attr.at[y, q], s.s_a.at[dy * NQ + dq],
                    s.r_a.at[dy * NQ + dq], z * NQ + qq, lax.rem(y + dy, NT),
                )
                c.start()
                a_copies.append(c)
    s.attr[y, q] = s.gbuf[q]
    for c in a_copies:
        c.wait_recv()
    parts = []
    for i in range(NQ):
        acc = s.attr[0, i].astype(F32)
        for t in range(1, NT):
            acc = acc + s.attr[t, i].astype(F32)
        parts.append(acc)
    lane32 = lane // 32
    tiles = []
    for zz in range(NZ):
        for h in range(2):
            tile = None
            for k in range(4):
                off = zz * 32
                piece = parts[h * 4 + k][:, (off // 128) * 128:(off // 128) * 128 + 128]
                shift = (k * 32 - off % 128) % 128
                if shift:
                    piece = pltpu.roll(piece, shift, 1)
                tile = piece if tile is None else jnp.where(lane32 == k, piece, tile)
            tiles.append(tile)
    x = s.tok_v[...].astype(F32) + jnp.concatenate(tiles, axis=1)
    mean = jnp.mean(x, axis=1, keepdims=True)
    xc = x - mean
    spread = jnp.mean(xc * xc, axis=1, keepdims=True)
    out[...] = (xc * lax.rsqrt(spread + EPS) * s.fg_v[...]).astype(BF16)
    for c in tok_copies + wg_copies + wo_copies + p_copies + n_copies + a_copies:
        c.wait_send()


def attention(tokens, lengths, keys, values, wq, wk, wv, mixw, hgain, wout, fgain):
    anywhere = pl.BlockSpec(memory_space=pl.ANY)
    smem = pl.BlockSpec(memory_space=pltpu.SMEM)
    return pl.pallas_call(
        attention_kernel,
        out_shape=jax.ShapeDtypeStruct((8, 2048), BF16),
        in_specs=[smem, smem] + [anywhere] * 9,
        out_specs=pl.BlockSpec(memory_space=pltpu.VMEM),
        scratch_shapes=list(A_SCRATCH.values()),
        compiler_params=pltpu.CompilerParams(
            collective_id=0, has_side_effects=True, vmem_limit_bytes=40 * 1024 * 1024
        ),
        name="attention",
    )(
        lengths, mixw, tokens, keys.reshape(8, 1024, 128), values.reshape(8, 1024, 128),
        wq, wk, wv, wout, hgain.reshape(1, 128), fgain.reshape(1, 2048),
    )


def in_one_piece(arrays, axis, dim, along):
    both = jnp.concatenate(arrays, axis=along)
    result, at, done = (lax.all_gather(both, axis, axis=dim, tiled=True), 0, [])
    for a in arrays:
        done.append(lax.slice_in_dim(result, at, at + a.shape[along], axis=along))
        at += a.shape[along]
    return tuple(done)


def laid_out(blocks, dim):
    blocks = jnp.moveaxis(blocks, 0, dim)
    lengths = blocks.shape
    return blocks.reshape(*lengths[:dim], lengths[dim] * lengths[dim + 1], *lengths[dim + 2 :])


def from_everyone(shard, axis):
    devices = lax.axis_size(axis)
    return lax.all_to_all(
        jnp.broadcast_to(shard[None], (devices, *shard.shape)), axis, 0, 0, tiled=True
    )


def gathered_copies(shard, axis, dim):
    return laid_out(from_everyone(shard, axis), dim)


def over_copies(shard, axis):
    return from_everyone(shard, axis).astype(jnp.float32).sum(axis=0)


def split_up(shard, dim, devices):
    lengths = shard.shape
    blocks = shard.reshape(*lengths[:dim], devices, lengths[dim] // devices, *lengths[dim + 1 :])
    return jnp.moveaxis(blocks, dim, 0)


def summed_on_arrival(shard, axis, dim):
    blocks = split_up(shard, dim, lax.axis_size(axis))
    arrived = lax.all_to_all(blocks, axis, split_axis=0, concat_axis=0, tiled=True)
    return arrived.astype(jnp.float32).sum(axis=0)


def of_everyone(shard, axis):
    everything = from_everyone(shard, axis)
    return jnp.sum(everything, axis=0)


def together(arrays, axis):
    ravelled, at, done = (jnp.concatenate([a.reshape(-1) for a in arrays]), 0, [])
    subtotal = of_everyone(ravelled, axis)
    for a in arrays:
        done.append(subtotal[at : at + a.size].reshape(a.shape))
        at += a.size
    return tuple(done)


def layer_norm(values, gain):
    mean = jnp.mean(values, axis=-1, keepdims=True)
    spread = jnp.mean(jnp.square(values - mean), axis=-1, keepdims=True)
    return (values - mean) * lax.rsqrt(spread + EPS) * gain


def body(
    tokens,
    lengths,
    cache_keys,
    cache_values,
    w_query,
    w_key,
    w_value,
    mix_weight,
    head_gain,
    w_out,
    first_gain,
    routing,
    route_weights,
    expert_gate,
    expert_up,
    expert_down,
    dense_gate,
    dense_up,
    dense_down,
    switch_vector,
    final_gain,
):
    f32 = jnp.float32
    bf16 = jnp.bfloat16
    seqs = tokens.shape[0]
    heads = mix_weight.shape[0]
    groups = cache_keys.shape[1]
    rep = heads // groups
    width = tokens.shape[1]
    hidden_state = attention(
        tokens, lengths, cache_keys, cache_values, w_query, w_key, w_value, mix_weight,
        head_gain, w_out, first_gain,
    )
    experts = lax.axis_size("ep") // SPAN
    capacity = min(seqs, max(2, 2 * seqs * TOP // experts))
    quarter = width // lax.axis_size("tp")
    offset = lax.axis_index("tp") * quarter
    own_slice = lax.dynamic_slice_in_dim(hidden_state, offset, quarter, 1)
    flat_route = routing.reshape(-1)
    chosen = (flat_route[:, None] == jnp.arange(experts, dtype=jnp.int32)[None, :]).astype(
        jnp.int32
    )
    slot_rank = jnp.sum((jnp.cumsum(chosen, axis=0) - 1) * chosen, axis=1)
    slot_hit = (slot_rank[:, None] == jnp.arange(capacity, dtype=jnp.int32)[None, :]).astype(
        jnp.int32
    )
    placing = chosen[:, :, None] * slot_hit[:, None, :]
    repeated = jnp.repeat(hidden_state, TOP, axis=0)
    packed = jnp.einsum(
        "rec,rd->ecd", placing.astype(bf16), repeated, preferred_element_type=f32
    ).astype(bf16)
    cols = packed.shape[-1]
    arrived = lax.all_to_all(
        jnp.broadcast_to(packed[:, None], (experts, SPAN, capacity, cols)).reshape(
            experts * SPAN, capacity, cols
        ),
        "ep",
        split_axis=0,
        concat_axis=0,
        tiled=True,
    )
    slots = arrived.shape[1]
    rows = arrived.reshape(-1, width)
    gate = jnp.dot(rows, expert_gate[0], preferred_element_type=f32)
    lift = jnp.dot(rows, expert_up[0], preferred_element_type=f32)
    local_hidden = (jax.nn.silu(gate) * lift).astype(bf16)
    full_hidden = gathered_copies(local_hidden, "tp", 1)
    block_out = jnp.dot(full_hidden, expert_down[0], preferred_element_type=f32).astype(bf16)
    block_out = block_out.reshape(arrived.shape[0], slots, block_out.shape[-1])
    returned = lax.all_to_all(block_out, "ep", split_axis=0, concat_axis=0, tiled=True)
    per_expert = jnp.sum(returned.astype(f32).reshape(experts, SPAN, capacity, quarter), axis=1)
    weighting = placing.astype(f32) * route_weights.reshape(-1)[:, None, None]
    routed = jnp.einsum("rec,ecd->rd", weighting, per_expert, precision=lax.Precision.HIGHEST)
    routed = jnp.sum(routed.reshape(seqs, TOP, quarter), axis=1)
    piece = gathered_copies(own_slice, "ep", 0)
    gate_part = jnp.dot(piece, dense_gate, preferred_element_type=f32)
    up_part = jnp.dot(piece, dense_up, preferred_element_type=f32)
    pre_gate, pre_up = (
        over_copies(gate_part.astype(jnp.bfloat16), "tp").astype(jnp.float32),
        over_copies(up_part.astype(jnp.bfloat16), "tp").astype(jnp.float32),
    )
    dense_hidden = (jax.nn.silu(pre_gate) * pre_up).astype(bf16)
    picked = dense_hidden
    dense_out = summed_on_arrival(
        jnp.dot(picked, dense_down, preferred_element_type=f32).astype(jnp.bfloat16), "ep", 0
    ).astype(bf16)
    switch = jax.nn.sigmoid(jnp.sum(hidden_state.astype(f32) * switch_vector, axis=-1))
    combined = own_slice.astype(f32) + routed + switch[:, None] * dense_out.astype(f32)
    sums, squares = together(
        (jnp.sum(combined, axis=-1), jnp.sum(combined * combined, axis=-1)), "tp"
    )
    mean = sums / width
    spread = squares / width - mean * mean
    result = (combined - mean[:, None]) * lax.rsqrt(spread[:, None] + EPS) * final_gain
    return result.astype(bf16)


def solution(mesh):
    placed = (
        P("ep", None),
        P("ep"),
        P("ep", "tp", None, None),
        P("ep", "tp", None, None),
        P("ep", "tp"),
        P("ep", "tp"),
        P("ep", "tp"),
        P("tp"),
        P(),
        P("tp", "ep"),
        P(),
        P("ep", None),
        P("ep", None),
        P("ep", None, "tp"),
        P("ep", None, "tp"),
        P("ep", None, "tp"),
        P("tp", "ep"),
        P("tp", "ep"),
        P("ep", "tp"),
        P(),
        P("tp"),
    )
    return jax.shard_map(body, mesh=mesh, in_specs=placed, out_specs=P("ep", "tp"), check_vma=False)
```

```python
from types import SimpleNamespace

import jax
import jax.numpy as jnp
import numpy as np
from jax import lax
from jax.experimental import pallas as pl
from jax.experimental.pallas import tpu as pltpu
from jax.sharding import PartitionSpec as P

EPS = 1e-05

NZ, NQ, NT = 8, 8, 4
MESH_ID = pl.DeviceIdType.MESH
F32 = jnp.float32
ONE = np.ones((2, 8), np.float32)
BF16 = jnp.bfloat16
NT_DIMS = (((1,), (1,)), ((), ()))


def dot(a, b):
    return jnp.dot(a, b, preferred_element_type=F32)


def dot_nt(a, b):
    return lax.dot_general(a, b, NT_DIMS, preferred_element_type=F32)


def stacked(ref, n):
    return jnp.concatenate([ref[i].astype(F32) for i in range(n)], axis=0).astype(BF16)


SCRATCH = dict(
    tok_v=pltpu.VMEM((8, 2048), BF16),
    tokg=pltpu.VMEM((NZ, 8, 256), BF16),
    wg=pltpu.VMEM((256, 768), BF16),
    wog=pltpu.VMEM((256, 512), BF16),
    kbuf=pltpu.VMEM((8, 1024, 128), BF16),
    vbuf=pltpu.VMEM((8, 1024, 128), BF16),
    fg_v=pltpu.VMEM((1, 2048), F32),
    hg_v=pltpu.VMEM((1, 128), F32),
    sw_v=pltpu.VMEM((1, 2048), F32),
    fin_v=pltpu.VMEM((1, 512), F32),
    pbuf=pltpu.VMEM((NZ, 8, 768), F32),
    precv=pltpu.VMEM((NZ, 8, 768), F32),
    qv=pltpu.VMEM((8, 768), F32),
    qs=pltpu.VMEM((8, 8, 128), F32),
    nv=pltpu.VMEM((8, 512), F32),
    ng=pltpu.VMEM((NQ, 8, 512), BF16),
    gbuf=pltpu.VMEM((NQ, 8, 256), BF16),
    attr=pltpu.VMEM((NT, NQ, 8, 256), BF16),
    eg=pltpu.VMEM((352, 2048), BF16),
    eu=pltpu.VMEM((352, 2048), BF16),
    ed=pltpu.VMEM((1408, 512), BF16),
    dw=pltpu.VMEM((3, 512, 512), BF16),
    hid=pltpu.VMEM((8, 2048), F32),
    sel=pltpu.VMEM((256, 256), BF16),
    selt=pltpu.VMEM((256, 256), BF16),
    pk=pltpu.VMEM((16, 8, 512), BF16),
    rows=pltpu.VMEM((2, 32, 8, 512), BF16),
    hg=pltpu.VMEM((2, NT, 64, 352), BF16),
    rb=pltpu.VMEM((2, 32, 8, 128), BF16),
    ret=pltpu.VMEM((64, 8, 128), BF16),
    dg=pltpu.VMEM((NZ, 8, 512), BF16),
    gp=pltpu.VMEM((NT, 16, 1024), BF16),
    gr=pltpu.VMEM((NT, 16, 1024), BF16),
    dh=pltpu.VMEM((NT, 16, 512), BF16),
    op=pltpu.VMEM((NZ, 8, 512), BF16),
    orv=pltpu.VMEM((NZ, 8, 512), BF16),
    st=pltpu.VMEM((NT, 8, 128), F32),
    lsem=pltpu.SemaphoreType.DMA((18,)),
    s_wg=pltpu.SemaphoreType.DMA((NQ,)),
    r_wg=pltpu.SemaphoreType.DMA((NQ,)),
    s_tok=pltpu.SemaphoreType.DMA((NZ,)),
    r_tok=pltpu.SemaphoreType.DMA((NZ,)),
    s_wo=pltpu.SemaphoreType.DMA((NZ,)),
    r_wo=pltpu.SemaphoreType.DMA((NZ,)),
    s_p=pltpu.SemaphoreType.DMA((NZ,)),
    r_p=pltpu.SemaphoreType.DMA((NZ,)),
    s_n=pltpu.SemaphoreType.DMA((NQ,)),
    r_n=pltpu.SemaphoreType.DMA((NQ,)),
    s_a=pltpu.SemaphoreType.DMA((NT * NQ,)),
    r_a=pltpu.SemaphoreType.DMA((NT * NQ,)),
    s_dw=pltpu.SemaphoreType.DMA((9,)),
    r_dw=pltpu.SemaphoreType.DMA((9,)),
    s_df=pltpu.SemaphoreType.DMA((3,)),
    r_df=pltpu.SemaphoreType.DMA((3,)),
    s_dp=pltpu.SemaphoreType.DMA((32,)),
    r_dp=pltpu.SemaphoreType.DMA((32,)),
    s_sw=pltpu.SemaphoreType.DMA((1,)),
    r_sw=pltpu.SemaphoreType.DMA((1,)),
    s_dg=pltpu.SemaphoreType.DMA((NZ,)),
    r_dg=pltpu.SemaphoreType.DMA((NZ,)),
    s_gr=pltpu.SemaphoreType.DMA((NT,)),
    r_gr=pltpu.SemaphoreType.DMA((NT,)),
    s_dh=pltpu.SemaphoreType.DMA((NT,)),
    r_dh=pltpu.SemaphoreType.DMA((NT,)),
    s_or=pltpu.SemaphoreType.DMA((NZ,)),
    r_or=pltpu.SemaphoreType.DMA((NZ,)),
    s_hg=pltpu.SemaphoreType.DMA((2 * NT,)),
    r_hg=pltpu.SemaphoreType.DMA((2 * NT,)),
    s_rt=pltpu.SemaphoreType.DMA((64,)),
    r_rt=pltpu.SemaphoreType.DMA((64,)),
    s_st=pltpu.SemaphoreType.DMA((NT,)),
    r_st=pltpu.SemaphoreType.DMA((NT,)),
)


def remote(src, dst, send, recv, ep, tp):
    return pltpu.make_async_remote_copy(
        src_ref=src, dst_ref=dst, send_sem=send, recv_sem=recv,
        device_id=(ep, tp), device_id_type=MESH_ID,
    )


def where_am_i():
    ep, tp = lax.axis_index("ep"), lax.axis_index("tp")
    return ep // NQ, lax.rem(ep, NQ), tp


def placing(e, slot, b, routing, weights):
    rank = jnp.zeros(e.shape, jnp.int32)
    share = jnp.zeros(e.shape, F32)
    for i in range(8):
        first, second = e == routing[0, i], e == routing[1, i]
        rank = rank + jnp.where((first | second) & (b > i), 1, 0)
        mine = jnp.where(first, weights[0, i], jnp.where(second, weights[1, i], 0.0))
        share = jnp.where(b == i, mine, share)
    return jnp.where(rank == slot, share, 0.0)


def silu(v):
    return v / (1.0 + jnp.exp(-v))


def iota2(shape):
    return tuple(lax.broadcasted_iota(jnp.int32, shape, i) for i in range(2))


def layer_kernel(
    lengths, mixw, routing, rweights, tokens, keys, values, wq, wk, wv, wout, hgain, fgain,
    egate, eup, edown, dgate, dup, ddown, switchv, final, out, *scratch
):
    s = SimpleNamespace(**dict(zip(SCRATCH, scratch)))
    z, q, y = where_am_i()
    x, core = q // 2, lax.rem(q, 2)
    me = z * NQ + q
    chip = me // 2
    sent = []

    def go(c):
        c.start()
        sent.append(c)
        return c

    qrow = pl.multiple_of(q * 32, 32)
    zrow = pl.multiple_of(z * 32, 32)
    first = [
        pltpu.make_async_copy(tokens, s.tok_v, s.lsem.at[0]),
        pltpu.make_async_copy(wq, s.wg.at[pl.ds(qrow, 32), pl.ds(0, 512)], s.lsem.at[1]),
        pltpu.make_async_copy(wk, s.wg.at[pl.ds(qrow, 32), pl.ds(512, 128)], s.lsem.at[2]),
        pltpu.make_async_copy(wv, s.wg.at[pl.ds(qrow, 32), pl.ds(640, 128)], s.lsem.at[3]),
        pltpu.make_async_copy(wout, s.wog.at[pl.ds(zrow, 32), :], s.lsem.at[4]),
    ]
    later = [
        pltpu.make_async_copy(keys, s.kbuf, s.lsem.at[5]),
        pltpu.make_async_copy(values, s.vbuf, s.lsem.at[6]),
        pltpu.make_async_copy(fgain, s.fg_v, s.lsem.at[7]),
        pltpu.make_async_copy(hgain, s.hg_v, s.lsem.at[8]),
    ]
    drow = pl.multiple_of((core * 4 + x) * 64, 64)
    dense = [
        pltpu.make_async_copy(w, s.dw.at[i, pl.ds(drow, 64), :], s.lsem.at[9 + i])
        for i, w in enumerate((dgate, dup, ddown))
    ]
    last = [
        pltpu.make_async_copy(egate, s.eg, s.lsem.at[12]),
        pltpu.make_async_copy(eup, s.eu, s.lsem.at[13]),
        pltpu.make_async_copy(edown, s.ed, s.lsem.at[14]),
        pltpu.make_async_copy(switchv, s.sw_v, s.lsem.at[15]),
        pltpu.make_async_copy(final, s.fin_v, s.lsem.at[16]),
    ]
    for c in first:
        c.start()

    barrier = pltpu.get_barrier_semaphore()
    for d in range(1, NZ):
        pl.semaphore_signal(
            barrier, inc=1, device_id=(lax.rem(z + d, NZ) * NQ + q, y), device_id_type=MESH_ID
        )
    for d in range(1, NQ):
        pl.semaphore_signal(
            barrier, inc=1, device_id=(z * NQ + lax.rem(q + d, NQ), y), device_id_type=MESH_ID
        )
    for d in range(1, NT):
        pl.semaphore_signal(
            barrier, inc=1, device_id=(me, lax.rem(y + d, NT)), device_id_type=MESH_ID
        )
    for c in dense + later + last:
        c.start()
    i, j = iota2((256, 256))
    s.sel[...] = jnp.where(j == (i % 32) * 8 + (i // 64) * 2 + (i // 32) % 2, 1.0, 0.0).astype(BF16)
    s.selt[...] = jnp.where(i == (j % 32) * 8 + (j // 64) * 2 + (j // 32) % 2, 1.0, 0.0).astype(BF16)
    for c in first + dense:
        c.wait()
    pl.semaphore_wait(barrier, NZ - 1 + NQ - 1 + NT - 1)

    wg_copies, tok_copies, wo_copies = [], [], []
    for d in range(1, NZ):
        zz = lax.rem(z + d, NZ)
        c = remote(
            s.tok_v.at[:, pl.ds(pl.multiple_of(zz * 256, 256), 256)], s.tokg.at[z],
            s.s_tok.at[d], s.r_tok.at[d], zz * NQ + q, y,
        )
        c.start()
        tok_copies.append(c)
    for d in range(1, NQ):
        mine = s.wg.at[pl.ds(qrow, 32), :]
        c = remote(mine, mine, s.s_wg.at[d], s.r_wg.at[d], z * NQ + lax.rem(q + d, NQ), y)
        c.start()
        wg_copies.append(c)
    for d in range(1, NZ):
        mine = s.wog.at[pl.ds(zrow, 32), :]
        c = remote(mine, mine, s.s_wo.at[d], s.r_wo.at[d], lax.rem(z + d, NZ) * NQ + q, y)
        c.start()
        wo_copies.append(c)
    dw_copies = []
    for i in range(3):
        for d in range(1, 4):
            mine = s.dw.at[i, pl.ds(drow, 64), :]
            k = i * 3 + d - 1
            dw_copies.append(go(remote(
                mine, mine, s.s_dw.at[k], s.r_dw.at[k], z * NQ + lax.rem(q + 2 * d, NQ), y
            )))
    s.tokg[z] = s.tok_v[:, pl.ds(pl.multiple_of(z * 256, 256), 256)]

    for c in tok_copies + wg_copies:
        c.wait_recv()
    part = dot(stacked(s.tokg, NZ), s.wg[...])
    for i in range(NZ):
        s.pbuf[i] = part[i * 8:(i + 1) * 8]
    p_copies = []
    for d in range(1, NZ):
        zz = lax.rem(z + d, NZ)
        c = remote(s.pbuf.at[zz], s.precv.at[z], s.s_p.at[d], s.r_p.at[d], zz * NQ + q, y)
        c.start()
        p_copies.append(c)
    s.precv[z] = s.pbuf[z]
    for c in p_copies:
        c.wait_recv()
    total = s.precv[0]
    for i in range(1, NZ):
        total = total + s.precv[i]
    s.qv[...] = total.astype(BF16).astype(F32)
    for b in range(8):
        for r in range(4):
            row = s.qv[b:b + 1, r * 128:(r + 1) * 128]
            s.qs[b, r:r + 1, :] = row
            s.qs[b, r + 4:r + 5, :] = row

    for c in later:
        c.wait()
    sub = lax.broadcasted_iota(jnp.int32, (8, 128), 0)
    lane = lax.broadcasted_iota(jnp.int32, (8, 128), 1)
    half = (sub >= 4) == (lane >= 64)
    col = lax.broadcasted_iota(jnp.int32, (8, 1024), 1)
    rows1 = lax.broadcasted_iota(jnp.int32, (8, 1), 0)
    lam = jnp.zeros((8, 1), F32)
    for r in range(4):
        lam = jnp.where(rows1 == r + 4, mixw[r], lam)
    weight = jnp.where(rows1 < 4, 1.0, -lam)
    for b in range(8):
        q8 = jnp.where(half, s.qs[b], 0.0)
        knew = s.qv[b:b + 1, 512:640]
        vnew = s.qv[b:b + 1, 640:768]
        sc = dot_nt(q8.astype(BF16), s.kbuf[b]) * 0.125
        own = jnp.sum(q8 * knew, axis=1, keepdims=True) * 0.125
        sc = jnp.where(col < lengths[b], sc, -jnp.inf)
        top = jnp.maximum(jnp.max(sc, axis=1, keepdims=True), own)
        e = jnp.exp(sc - top)
        eo = jnp.exp(own - top)
        scale = weight / (jnp.sum(e, axis=1, keepdims=True) + eo)
        t = e * scale
        mix = (t + pltpu.roll(t, 4, 0)).astype(BF16)
        to = jnp.broadcast_to(eo * scale, (8, 128))
        mix_own = (to + pltpu.roll(to, 4, 0)).astype(BF16).astype(F32)
        ho = dot(mix, s.vbuf[b]) + mix_own * vnew
        square = jnp.mean(ho * ho, axis=1, keepdims=True)
        n8 = ho * lax.rsqrt(square + EPS) * s.hg_v[...]
        for r in range(4):
            s.nv[b:b + 1, r * 128:(r + 1) * 128] = n8[r:r + 1, :]
    s.ng[q] = s.nv[...].astype(BF16)
    n_copies = []
    for d in range(1, NQ):
        c = remote(
            s.ng.at[q], s.ng.at[q], s.s_n.at[d], s.r_n.at[d], z * NQ + lax.rem(q + d, NQ), y
        )
        c.start()
        n_copies.append(c)
    for c in wo_copies + n_copies:
        c.wait_recv()
    group = dot_nt(stacked(s.ng, NQ), s.wog[...])
    for i in range(NQ):
        s.gbuf[i] = group[i * 8:(i + 1) * 8].astype(BF16)
    a_copies = []
    for dy in range(NT):
        for dq in range(NQ):
            if dy or dq:
                qq = lax.rem(q + dq, NQ)
                c = remote(
                    s.gbuf.at[qq], s.attr.at[y, q], s.s_a.at[dy * NQ + dq],
                    s.r_a.at[dy * NQ + dq], z * NQ + qq, lax.rem(y + dy, NT),
                )
                c.start()
                a_copies.append(c)
    s.attr[y, q] = s.gbuf[q]
    for c in dw_copies:
        c.wait_recv()
    df_copies = []
    other = me + 1 - 2 * core
    for i in range(3):
        mine = s.dw.at[i, pl.ds(pl.multiple_of(core * 256, 256), 256), :]
        df_copies.append(go(remote(mine, mine, s.s_df.at[i], s.r_df.at[i], other, y)))
    for c in a_copies:
        c.wait_recv()
    parts = []
    for i in range(NQ):
        acc = s.attr[0, i].astype(F32)
        for t in range(1, NT):
            acc = acc + s.attr[t, i].astype(F32)
        parts.append(acc)
    lane32 = lane // 32
    tiles = []
    for zz in range(NZ):
        for h in range(2):
            tile = None
            for k in range(4):
                off = zz * 32
                piece = parts[h * 4 + k][:, (off // 128) * 128:(off // 128) * 128 + 128]
                shift = (k * 32 - off % 128) % 128
                if shift:
                    piece = pltpu.roll(piece, shift, 1)
                tile = piece if tile is None else jnp.where(lane32 == k, piece, tile)
            tiles.append(tile)
    x = s.tok_v[...].astype(F32) + jnp.concatenate(tiles, axis=1)
    mean = jnp.mean(x, axis=1, keepdims=True)
    xc = x - mean
    spread = jnp.mean(xc * xc, axis=1, keepdims=True)
    hidden = (xc * lax.rsqrt(spread + EPS) * s.fg_v[...]).astype(BF16)
    hid32 = hidden.astype(F32)
    s.hid[...] = hid32

    i, j = iota2((128, 32))
    ones = placing(i // 8, i % 2, j % 8, routing, ONE)
    place = jnp.where((i // 2) % 4 == j // 8, ones, 0.0).astype(BF16)
    quarters = jnp.concatenate([hid32[:, t * 512:(t + 1) * 512] for t in range(4)], axis=0)
    packed = dot(place, quarters.astype(BF16))
    for e in range(16):
        s.pk[e] = packed[e * 8:(e + 1) * 8].astype(BF16)
    dp_copies = []
    for d in range(1, 32):
        to = lax.rem(chip + d, 32)
        dp_copies.append(go(remote(
            s.pk.at[to // 2], s.rows.at[0, chip], s.s_dp.at[d], s.r_dp.at[d], to * 2 + core, y
        )))
    s.rows[0, chip] = s.pk[chip // 2]

    s.dg[z] = s.hid[:, pl.ds(pl.multiple_of(y * 512, 512), 512)].astype(BF16)
    dg_copies = [
        go(remote(
            s.dg.at[z], s.dg.at[z], s.s_dg.at[d], s.r_dg.at[d], lax.rem(z + d, NZ) * NQ + q, y
        ))
        for d in range(1, NZ)
    ]
    for c in last:
        c.wait()
    i, j = iota2((32, 128))
    shares = placing(j // 8, j % 2, i % 8, routing, rweights)
    shares = jnp.where((j // 2) % 4 == i // 8, shares, 0.0)
    switch = 1.0 / (1.0 + jnp.exp(-jnp.sum(hid32 * s.sw_v[...], axis=1, keepdims=True)))

    for c in df_copies + dg_copies:
        c.wait_recv()
    group = stacked(s.dg, NZ)
    for k in range(2):
        part = dot_nt(group, s.dw[k]).astype(BF16)
        for t in range(NT):
            s.gp[t, :, k * 512:(k + 1) * 512] = part[t * 16:(t + 1) * 16]
    gr_copies = []
    for d in range(1, NT):
        to = lax.rem(y + d, NT)
        gr_copies.append(go(remote(
            s.gp.at[to], s.gr.at[y], s.s_gr.at[d], s.r_gr.at[d], me, to
        )))
    s.gr[y] = s.gp[y]

    def expert_half(h):
        block = dot(s.sel[...], jnp.concatenate(
            [s.rows[h, i].astype(F32) for i in range(32)], axis=0).astype(BF16)).astype(BF16)
        wide = jnp.concatenate([block[t * 64:(t + 1) * 64] for t in range(4)], axis=1)
        gate, up = dot_nt(wide, s.eg[...]), dot_nt(wide, s.eu[...])
        s.hg[h, y] = (silu(gate) * up).astype(BF16)
        return [
            go(remote(
                s.hg.at[h, y], s.hg.at[h, y], s.s_hg.at[h * NT + d], s.r_hg.at[h * NT + d],
                me, lax.rem(y + d, NT),
            ))
            for d in range(1, NT)
        ]

    for c in dp_copies:
        c.wait_recv()
    swap = go(remote(s.rows.at[0], s.rows.at[1], s.s_sw.at[0], s.r_sw.at[0], other, y))
    hg_copies = [expert_half(0)]

    for c in gr_copies:
        c.wait_recv()
    pre = s.gr[0].astype(F32)
    for t in range(1, NT):
        pre = pre + s.gr[t].astype(F32)
    s.dh[y] = (silu(pre[:, :512]) * pre[:, 512:]).astype(BF16)
    dh_copies = [
        go(remote(
            s.dh.at[y], s.dh.at[y], s.s_dh.at[d], s.r_dh.at[d], me, lax.rem(y + d, NT)
        ))
        for d in range(1, NT)
    ]

    swap.wait_recv()
    hg_copies.append(expert_half(1))

    for c in dh_copies:
        c.wait_recv()
    part = dot(jnp.concatenate([s.dh[t] for t in range(NT)], axis=0), s.dw[2])
    for i in range(NZ):
        s.op[i] = part[i * 8:(i + 1) * 8].astype(BF16)
    or_copies = []
    for d in range(1, NZ):
        to = lax.rem(z + d, NZ)
        or_copies.append(go(remote(
            s.op.at[to], s.orv.at[z], s.s_or.at[d], s.r_or.at[d], to * NQ + q, y
        )))
    s.orv[z] = s.op[z]

    rt_copies = []
    for h in range(2):
        for c in hg_copies[h]:
            c.wait_recv()
        acc = dot(s.hg[h, 0], s.ed[0:352])
        for t in range(1, NT):
            acc = acc + dot(s.hg[h, t], s.ed[t * 352:(t + 1) * 352])
        acc = acc.astype(BF16)
        tall = jnp.concatenate([acc[:, t * 128:(t + 1) * 128] for t in range(4)], axis=0)
        back = dot(s.selt[...], tall)
        for i in range(32):
            s.rb[h, i] = back[i * 8:(i + 1) * 8].astype(BF16)
        there = core if h == 0 else 1 - core
        for d in range(32):
            to = lax.rem(chip + d, 32)
            if h or d:
                k = h * 32 + d
                rt_copies.append(go(remote(
                    s.rb.at[h, to], s.ret.at[me], s.s_rt.at[k], s.r_rt.at[k], to * 2 + there, y
                )))
            else:
                s.ret[me] = s.rb[0, chip]

    for c in or_copies:
        c.wait_recv()
    dense_out = s.orv[0].astype(F32)
    for i in range(1, NZ):
        dense_out = dense_out + s.orv[i].astype(F32)
    dense_out = dense_out.astype(BF16).astype(F32)
    combined = s.hid[:, pl.ds(pl.multiple_of(y * 512, 512), 512)] + switch * dense_out

    for c in rt_copies:
        c.wait_recv()
    sums = []
    for e in range(16):
        acc = s.ret[4 * e].astype(F32)
        for t in range(1, 4):
            acc = acc + s.ret[4 * e + t].astype(F32)
        sums.append(acc)
    routed = jnp.dot(
        shares, jnp.concatenate(sums, axis=0), preferred_element_type=F32,
        precision=lax.Precision.HIGHEST,
    )
    combined = combined + jnp.concatenate([routed[t * 8:(t + 1) * 8] for t in range(4)], axis=1)
    total = jnp.sum(combined, axis=1, keepdims=True)
    square = jnp.sum(combined * combined, axis=1, keepdims=True)
    s.st[y] = jnp.where(lane < 64, total, square)
    st_copies = [
        go(remote(
            s.st.at[y], s.st.at[y], s.s_st.at[d], s.r_st.at[d], me, lax.rem(y + d, NT)
        ))
        for d in range(1, NT)
    ]
    for c in st_copies:
        c.wait_recv()
    stats = s.st[0] + s.st[1] + s.st[2] + s.st[3]
    mean = stats[:, 0:1] / 2048
    spread = stats[:, 64:65] / 2048 - mean * mean
    result = (combined - mean) * lax.rsqrt(spread + EPS) * s.fin_v[...]
    out[...] = result.astype(BF16)
    for c in tok_copies + wg_copies + wo_copies + p_copies + n_copies + a_copies + sent:
        c.wait_send()


def body(
    tokens, lengths, cache_keys, cache_values, w_query, w_key, w_value, mix_weight, head_gain,
    w_out, first_gain, routing, route_weights, expert_gate, expert_up, expert_down, dense_gate,
    dense_up, dense_down, switch_vector, final_gain,
):
    hbm = pl.BlockSpec(memory_space=pltpu.HBM)
    smem = pl.BlockSpec(memory_space=pltpu.SMEM)
    return pl.pallas_call(
        layer_kernel,
        out_shape=jax.ShapeDtypeStruct((8, 512), BF16),
        in_specs=[smem] * 4 + [hbm] * 17,
        out_specs=pl.BlockSpec(memory_space=pltpu.VMEM),
        scratch_shapes=list(SCRATCH.values()),
        compiler_params=pltpu.CompilerParams(
            collective_id=0, has_side_effects=True, vmem_limit_bytes=60 * 1024 * 1024
        ),
        name="layer",
    )(
        lengths, mix_weight, routing.T, route_weights.T, tokens,
        cache_keys.reshape(8, 1024, 128), cache_values.reshape(8, 1024, 128),
        w_query, w_key, w_value, w_out.T, head_gain.reshape(1, 128),
        first_gain.reshape(1, 2048), expert_gate[0].T, expert_up[0].T, expert_down[0],
        dense_gate.T, dense_up.T, dense_down, switch_vector.reshape(1, 2048),
        final_gain.reshape(1, 512),
    )


def solution(mesh):
    placed = (
        P("ep", None),
        P("ep"),
        P("ep", "tp", None, None),
        P("ep", "tp", None, None),
        P("ep", "tp"),
        P("ep", "tp"),
        P("ep", "tp"),
        P("tp"),
        P(),
        P("tp", "ep"),
        P(),
        P("ep", None),
        P("ep", None),
        P("ep", None, "tp"),
        P("ep", None, "tp"),
        P("ep", None, "tp"),
        P("tp", "ep"),
        P("tp", "ep"),
        P("ep", "tp"),
        P(),
        P("tp"),
    )
    return jax.shard_map(body, mesh=mesh, in_specs=placed, out_specs=P("ep", "tp"), check_vma=False)
```

```python
from types import SimpleNamespace

import jax
import jax.numpy as jnp
import numpy as np
from jax import lax
from jax.experimental import pallas as pl
from jax.experimental.pallas import tpu as pltpu
from jax.sharding import PartitionSpec as P

EPS = 1e-05

NZ, NQ, NT = 8, 8, 4
FAR_Z = (4, 3, 5, 2, 6, 1, 7)
FAR_Q = (4, 5, 3, 2, 6, 7, 1)
FAR_X = (2, 1, 3)
FAR_T = (2, 1, 3)
MESH_ID = pl.DeviceIdType.MESH
F32 = jnp.float32
ONE = np.ones((2, 8), np.float32)
BF16 = jnp.bfloat16
NT_DIMS = (((1,), (1,)), ((), ()))


def dot(a, b):
    return jnp.dot(a, b, preferred_element_type=F32)


def dot_nt(a, b):
    return lax.dot_general(a, b, NT_DIMS, preferred_element_type=F32)


def stacked(ref, n):
    return jnp.concatenate([ref[i].astype(F32) for i in range(n)], axis=0).astype(BF16)


SCRATCH = dict(
    tok_v=pltpu.VMEM((8, 2048), BF16),
    tokg=pltpu.VMEM((2 * NZ, 8, 256), BF16),
    wmine=pltpu.VMEM((32, 768), BF16),
    wg=pltpu.VMEM((256, 384), BF16),
    wog=pltpu.VMEM((256, 512), BF16),
    kbuf=pltpu.VMEM((8, 1024, 128), BF16),
    vbuf=pltpu.VMEM((8, 1024, 128), BF16),
    fg_v=pltpu.VMEM((1, 2048), F32),
    hg_v=pltpu.VMEM((1, 128), F32),
    sw_v=pltpu.VMEM((1, 2048), F32),
    fin_v=pltpu.VMEM((1, 512), F32),
    pbuf=pltpu.VMEM((2 * NZ, 8, 384), F32),
    precv=pltpu.VMEM((2, NZ, 8, 384), F32),
    qv=pltpu.VMEM((8, 768), F32),
    qs=pltpu.VMEM((8, 8, 128), F32),
    nv=pltpu.VMEM((8, 512), F32),
    ng=pltpu.VMEM((NQ, 8, 512), BF16),
    gbuf=pltpu.VMEM((NQ, 8, 256), BF16),
    attr=pltpu.VMEM((NT, NQ, 8, 256), BF16),
    eg=pltpu.VMEM((352, 2048), BF16),
    eu=pltpu.VMEM((352, 2048), BF16),
    ed=pltpu.VMEM((1408, 512), BF16),
    dw=pltpu.VMEM((3, 512, 512), BF16),
    hid=pltpu.VMEM((8, 2048), F32),
    sel=pltpu.VMEM((256, 256), BF16),
    selt=pltpu.VMEM((256, 256), BF16),
    pk=pltpu.VMEM((16, 8, 512), BF16),
    rows=pltpu.VMEM((2, 32, 8, 512), BF16),
    hg=pltpu.VMEM((2, NT, 64, 352), BF16),
    rb=pltpu.VMEM((2, 32, 8, 128), BF16),
    ret=pltpu.VMEM((64, 8, 128), BF16),
    dg=pltpu.VMEM((NZ, 8, 512), BF16),
    gp=pltpu.VMEM((NT, 16, 1024), BF16),
    gr=pltpu.VMEM((NT, 16, 1024), BF16),
    dh=pltpu.VMEM((NT, 16, 512), BF16),
    op=pltpu.VMEM((NZ, 8, 512), BF16),
    orv=pltpu.VMEM((NZ, 8, 512), BF16),
    st=pltpu.VMEM((NT, 8, 128), F32),
    len_s=pltpu.SMEM((8,), jnp.int32),
    mix_s=pltpu.SMEM((4,), F32),
    rt_s=pltpu.SMEM((2, 8), jnp.int32),
    rw_s=pltpu.SMEM((2, 8), F32),
    lsem=pltpu.SemaphoreType.DMA((21,)),
    s_wg=pltpu.SemaphoreType.DMA((NQ,)),
    r_wg=pltpu.SemaphoreType.DMA((NQ,)),
    s_tok=pltpu.SemaphoreType.DMA((2 * NZ,)),
    r_tok=pltpu.SemaphoreType.DMA((2 * NZ,)),
    s_wo=pltpu.SemaphoreType.DMA((NZ,)),
    r_wo=pltpu.SemaphoreType.DMA((NZ,)),
    s_p=pltpu.SemaphoreType.DMA((2 * NZ,)),
    r_p=pltpu.SemaphoreType.DMA((2 * NZ,)),
    s_n=pltpu.SemaphoreType.DMA((NQ,)),
    r_n=pltpu.SemaphoreType.DMA((NQ,)),
    s_a=pltpu.SemaphoreType.DMA((NT * NQ,)),
    r_a=pltpu.SemaphoreType.DMA((NT * NQ,)),
    s_dw=pltpu.SemaphoreType.DMA((9,)),
    r_dw=pltpu.SemaphoreType.DMA((9,)),
    s_df=pltpu.SemaphoreType.DMA((3,)),
    r_df=pltpu.SemaphoreType.DMA((3,)),
    s_dp=pltpu.SemaphoreType.DMA((32,)),
    r_dp=pltpu.SemaphoreType.DMA((32,)),
    s_sw=pltpu.SemaphoreType.DMA((1,)),
    r_sw=pltpu.SemaphoreType.DMA((1,)),
    s_dg=pltpu.SemaphoreType.DMA((NZ,)),
    r_dg=pltpu.SemaphoreType.DMA((NZ,)),
    s_gr=pltpu.SemaphoreType.DMA((NT,)),
    r_gr=pltpu.SemaphoreType.DMA((NT,)),
    s_dh=pltpu.SemaphoreType.DMA((NT,)),
    r_dh=pltpu.SemaphoreType.DMA((NT,)),
    s_or=pltpu.SemaphoreType.DMA((NZ,)),
    r_or=pltpu.SemaphoreType.DMA((NZ,)),
    s_hg=pltpu.SemaphoreType.DMA((2 * NT,)),
    r_hg=pltpu.SemaphoreType.DMA((2 * NT,)),
    s_rt=pltpu.SemaphoreType.DMA((64,)),
    r_rt=pltpu.SemaphoreType.DMA((64,)),
    s_st=pltpu.SemaphoreType.DMA((NT,)),
    r_st=pltpu.SemaphoreType.DMA((NT,)),
)


def remote(src, dst, send, recv, ep, tp):
    return pltpu.make_async_remote_copy(
        src_ref=src, dst_ref=dst, send_sem=send, recv_sem=recv,
        device_id=(ep, tp), device_id_type=MESH_ID,
    )


def where_am_i():
    ep, tp = lax.axis_index("ep"), lax.axis_index("tp")
    return ep // NQ, lax.rem(ep, NQ), tp


def placing(e, slot, b, routing, weights):
    rank = jnp.zeros(e.shape, jnp.int32)
    share = jnp.zeros(e.shape, F32)
    for i in range(8):
        first, second = e == routing[0, i], e == routing[1, i]
        rank = rank + jnp.where((first | second) & (b > i), 1, 0)
        mine = jnp.where(first, weights[0, i], jnp.where(second, weights[1, i], 0.0))
        share = jnp.where(b == i, mine, share)
    return jnp.where(rank == slot, share, 0.0)


def silu(v):
    return v / (1.0 + jnp.exp(-v))


def iota2(shape):
    return tuple(lax.broadcasted_iota(jnp.int32, shape, i) for i in range(2))


def layer_kernel(
    lengths, mixw, routing, rweights, tokens, keys, values, wq, wk, wv, wout, hgain, fgain,
    egate, eup, edown, dgate, dup, ddown, switchv, final, out, *scratch
):
    s = SimpleNamespace(**dict(zip(SCRATCH, scratch)))
    z, q, y = where_am_i()
    x, core = q // 2, lax.rem(q, 2)
    me = z * NQ + q
    chip = me // 2
    sent = []

    def go(c):
        c.start()
        sent.append(c)
        return c

    qrow = pl.multiple_of(q * 32, 32)
    zrow = pl.multiple_of(z * 32, 32)
    first = [
        pltpu.make_async_copy(tokens, s.tok_v, s.lsem.at[0]),
        pltpu.make_async_copy(wq, s.wmine.at[:, pl.ds(0, 512)], s.lsem.at[1]),
        pltpu.make_async_copy(wk, s.wmine.at[:, pl.ds(512, 128)], s.lsem.at[2]),
        pltpu.make_async_copy(wv, s.wmine.at[:, pl.ds(640, 128)], s.lsem.at[3]),
        pltpu.make_async_copy(wout, s.wog.at[pl.ds(zrow, 32), :], s.lsem.at[4]),
    ]
    later = [
        pltpu.make_async_copy(keys, s.kbuf, s.lsem.at[5]),
        pltpu.make_async_copy(values, s.vbuf, s.lsem.at[6]),
        pltpu.make_async_copy(fgain, s.fg_v, s.lsem.at[7]),
        pltpu.make_async_copy(hgain, s.hg_v, s.lsem.at[8]),
        pltpu.make_async_copy(lengths, s.len_s, s.lsem.at[17]),
        pltpu.make_async_copy(mixw, s.mix_s, s.lsem.at[18]),
        pltpu.make_async_copy(routing, s.rt_s, s.lsem.at[19]),
        pltpu.make_async_copy(rweights, s.rw_s, s.lsem.at[20]),
    ]
    drow = pl.multiple_of((core * 4 + x) * 64, 64)
    dense = [
        pltpu.make_async_copy(w, s.dw.at[i, pl.ds(drow, 64), :], s.lsem.at[9 + i])
        for i, w in enumerate((dgate, dup, ddown))
    ]
    last = [
        pltpu.make_async_copy(egate, s.eg, s.lsem.at[12]),
        pltpu.make_async_copy(eup, s.eu, s.lsem.at[13]),
        pltpu.make_async_copy(edown, s.ed, s.lsem.at[14]),
        pltpu.make_async_copy(switchv, s.sw_v, s.lsem.at[15]),
        pltpu.make_async_copy(final, s.fin_v, s.lsem.at[16]),
    ]
    for c in first:
        c.start()

    barrier = pltpu.get_barrier_semaphore()
    for d in FAR_Z:
        for swap in range(2):
            to = lax.rem(z + d, NZ) * NQ + x * 2 + lax.rem(core + swap, 2)
            pl.semaphore_signal(barrier, inc=1, device_id=(to, y), device_id_type=MESH_ID)
    for d in FAR_Q:
        pl.semaphore_signal(
            barrier, inc=1, device_id=(z * NQ + lax.rem(q + d, NQ), y), device_id_type=MESH_ID
        )
    for d in FAR_T:
        pl.semaphore_signal(
            barrier, inc=1, device_id=(me, lax.rem(y + d, NT)), device_id_type=MESH_ID
        )
    for c in dense + later:
        c.start()
    i, j = iota2((256, 256))
    s.sel[...] = jnp.where(j == (i % 32) * 8 + (i // 64) * 2 + (i // 32) % 2, 1.0, 0.0).astype(BF16)
    s.selt[...] = jnp.where(i == (j % 32) * 8 + (j // 64) * 2 + (j // 32) % 2, 1.0, 0.0).astype(BF16)
    for c in first:
        c.wait()
    half = pl.ds(pl.multiple_of(core * 384, 384), 384)
    s.wg[pl.ds(qrow, 32), :] = s.wmine[:, half]
    s.tokg[z * 2 + core] = s.tok_v[:, pl.ds(pl.multiple_of(z * 256, 256), 256)]
    pl.semaphore_wait(barrier, 2 * (NZ - 1) + NQ - 1 + NT - 1)

    wg_copies, tok_copies, wo_copies = [], [], []
    for d in FAR_Q:
        to = lax.rem(q + d, NQ)
        theirs = pl.ds(pl.multiple_of(lax.rem(to, 2) * 384, 384), 384)
        wg_copies.append(go(remote(
            s.wmine.at[:, theirs], s.wg.at[pl.ds(qrow, 32), :], s.s_wg.at[d], s.r_wg.at[d],
            z * NQ + to, y,
        )))
    for d in FAR_Z + (0,):
        for swap in range(2):
            if d or swap:
                zz, k = lax.rem(z + d, NZ), d * 2 + swap
                tok_copies.append(go(remote(
                    s.tok_v.at[:, pl.ds(pl.multiple_of(zz * 256, 256), 256)],
                    s.tokg.at[z * 2 + core], s.s_tok.at[k], s.r_tok.at[k],
                    zz * NQ + x * 2 + lax.rem(core + swap, 2), y,
                )))
    for c in last:
        c.start()

    for c in tok_copies + wg_copies:
        c.wait_recv()
    part = dot(stacked(s.tokg, 2 * NZ), s.wg[...])
    for i in range(2 * NZ):
        s.pbuf[i] = part[i * 8:(i + 1) * 8]
    p_copies = []
    for d in FAR_Z + (0,):
        for swap in range(2):
            if d or swap:
                zz, k = lax.rem(z + d, NZ), d * 2 + swap
                cc = lax.rem(core + swap, 2)
                p_copies.append(go(remote(
                    s.pbuf.at[zz * 2 + cc], s.precv.at[core, z], s.s_p.at[k], s.r_p.at[k],
                    zz * NQ + x * 2 + cc, y,
                )))
    for d in FAR_Z:
        mine = s.wog.at[pl.ds(zrow, 32), :]
        wo_copies.append(go(remote(
            mine, mine, s.s_wo.at[d], s.r_wo.at[d], lax.rem(z + d, NZ) * NQ + q, y
        )))
    for c in dense:
        c.wait()
    dw_copies = []
    for i in range(3):
        for d in FAR_X:
            mine = s.dw.at[i, pl.ds(drow, 64), :]
            k = i * 3 + d - 1
            dw_copies.append(go(remote(
                mine, mine, s.s_dw.at[k], s.r_dw.at[k], z * NQ + lax.rem(q + 2 * d, NQ), y
            )))
    s.precv[core, z] = s.pbuf[z * 2 + core]
    for c in p_copies:
        c.wait_recv()
    sides = []
    for h in range(2):
        side = s.precv[h, 0]
        for i in range(1, NZ):
            side = side + s.precv[h, i]
        sides.append(side)
    total = jnp.concatenate(sides, axis=1)
    s.qv[...] = total.astype(BF16).astype(F32)
    for b in range(8):
        for r in range(4):
            row = s.qv[b:b + 1, r * 128:(r + 1) * 128]
            s.qs[b, r:r + 1, :] = row
            s.qs[b, r + 4:r + 5, :] = row

    for c in later:
        c.wait()
    sub = lax.broadcasted_iota(jnp.int32, (8, 128), 0)
    lane = lax.broadcasted_iota(jnp.int32, (8, 128), 1)
    own_half = (sub >= 4) == (lane >= 64)
    col = lax.broadcasted_iota(jnp.int32, (8, 1024), 1)
    rows1 = lax.broadcasted_iota(jnp.int32, (8, 1), 0)
    lam = jnp.zeros((8, 1), F32)
    for r in range(4):
        lam = jnp.where(rows1 == r + 4, s.mix_s[r], lam)
    weight = jnp.where(rows1 < 4, 1.0, -lam)
    for b in range(8):
        q8 = jnp.where(own_half, s.qs[b], 0.0)
        knew = s.qv[b:b + 1, 512:640]
        vnew = s.qv[b:b + 1, 640:768]
        sc = dot_nt(q8.astype(BF16), s.kbuf[b]) * 0.125
        own = jnp.sum(q8 * knew, axis=1, keepdims=True) * 0.125
        sc = jnp.where(col < s.len_s[b], sc, -jnp.inf)
        top = jnp.maximum(jnp.max(sc, axis=1, keepdims=True), own)
        e = jnp.exp(sc - top)
        eo = jnp.exp(own - top)
        scale = weight / (jnp.sum(e, axis=1, keepdims=True) + eo)
        t = e * scale
        mix = (t + pltpu.roll(t, 4, 0)).astype(BF16)
        to = jnp.broadcast_to(eo * scale, (8, 128))
        mix_own = (to + pltpu.roll(to, 4, 0)).astype(BF16).astype(F32)
        ho = dot(mix, s.vbuf[b]) + mix_own * vnew
        square = jnp.mean(ho * ho, axis=1, keepdims=True)
        n8 = ho * lax.rsqrt(square + EPS) * s.hg_v[...]
        for r in range(4):
            s.nv[b:b + 1, r * 128:(r + 1) * 128] = n8[r:r + 1, :]
    s.ng[q] = s.nv[...].astype(BF16)
    n_copies = []
    for d in FAR_Q:
        c = go(remote(
            s.ng.at[q], s.ng.at[q], s.s_n.at[d], s.r_n.at[d], z * NQ + lax.rem(q + d, NQ), y
        ))
        n_copies.append(c)
    for c in wo_copies + n_copies:
        c.wait_recv()
    group = dot_nt(stacked(s.ng, NQ), s.wog[...])
    for i in range(NQ):
        s.gbuf[i] = group[i * 8:(i + 1) * 8].astype(BF16)
    a_copies = []
    for dq in FAR_Q + (0,):
        for dy in FAR_T + (0,):
            if dy or dq:
                qq = lax.rem(q + dq, NQ)
                c = go(remote(
                    s.gbuf.at[qq], s.attr.at[y, q], s.s_a.at[dy * NQ + dq],
                    s.r_a.at[dy * NQ + dq], z * NQ + qq, lax.rem(y + dy, NT),
                ))
                a_copies.append(c)
    s.attr[y, q] = s.gbuf[q]
    for c in a_copies:
        c.wait_recv()
    parts = []
    for i in range(NQ):
        acc = s.attr[0, i].astype(F32)
        for t in range(1, NT):
            acc = acc + s.attr[t, i].astype(F32)
        parts.append(acc)
    lane32 = lane // 32
    tiles = []
    for zz in range(NZ):
        for h in range(2):
            tile = None
            for k in range(4):
                off = zz * 32
                piece = parts[h * 4 + k][:, (off // 128) * 128:(off // 128) * 128 + 128]
                shift = (k * 32 - off % 128) % 128
                if shift:
                    piece = pltpu.roll(piece, shift, 1)
                tile = piece if tile is None else jnp.where(lane32 == k, piece, tile)
            tiles.append(tile)
    state = s.tok_v[...].astype(F32) + jnp.concatenate(tiles, axis=1)
    mean = jnp.mean(state, axis=1, keepdims=True)
    xc = state - mean
    spread = jnp.mean(xc * xc, axis=1, keepdims=True)
    hidden = (xc * lax.rsqrt(spread + EPS) * s.fg_v[...]).astype(BF16)
    hid32 = hidden.astype(F32)
    s.hid[...] = hid32

    i, j = iota2((128, 32))
    ones = placing(i // 8, i % 2, j % 8, s.rt_s, ONE)
    place = jnp.where((i // 2) % 4 == j // 8, ones, 0.0).astype(BF16)
    quarters = jnp.concatenate([hid32[:, t * 512:(t + 1) * 512] for t in range(4)], axis=0)
    packed = dot(place, quarters.astype(BF16))
    for e in range(16):
        s.pk[e] = packed[e * 8:(e + 1) * 8].astype(BF16)
    dp_copies = []
    for dx in FAR_X + (0,):
        for dz in FAR_Z + (0,):
            if dx or dz:
                to, k = lax.rem(z + dz, NZ) * 4 + lax.rem(x + dx, 4), dz * 4 + dx
                dp_copies.append(go(remote(
                    s.pk.at[to // 2], s.rows.at[0, chip], s.s_dp.at[k], s.r_dp.at[k],
                    to * 2 + core, y,
                )))
    s.rows[0, chip] = s.pk[chip // 2]

    s.dg[z] = s.hid[:, pl.ds(pl.multiple_of(y * 512, 512), 512)].astype(BF16)
    dg_copies = [
        go(remote(
            s.dg.at[z], s.dg.at[z], s.s_dg.at[d], s.r_dg.at[d], lax.rem(z + d, NZ) * NQ + q, y
        ))
        for d in FAR_Z
    ]
    for c in dw_copies:
        c.wait_recv()
    other = me + 1 - 2 * core
    df_copies = []
    for i in range(3):
        mine = s.dw.at[i, pl.ds(pl.multiple_of(core * 256, 256), 256), :]
        df_copies.append(go(remote(mine, mine, s.s_df.at[i], s.r_df.at[i], other, y)))
    for c in last:
        c.wait()
    i, j = iota2((32, 128))
    shares = placing(j // 8, j % 2, i % 8, s.rt_s, s.rw_s)
    shares = jnp.where((j // 2) % 4 == i // 8, shares, 0.0)
    switch = 1.0 / (1.0 + jnp.exp(-jnp.sum(hid32 * s.sw_v[...], axis=1, keepdims=True)))

    def expert_half(h):
        block = dot(s.sel[...], jnp.concatenate(
            [s.rows[h, i].astype(F32) for i in range(32)], axis=0).astype(BF16)).astype(BF16)
        wide = jnp.concatenate([block[t * 64:(t + 1) * 64] for t in range(4)], axis=1)
        gate, up = dot_nt(wide, s.eg[...]), dot_nt(wide, s.eu[...])
        s.hg[h, y] = (silu(gate) * up).astype(BF16)
        return [
            go(remote(
                s.hg.at[h, y], s.hg.at[h, y], s.s_hg.at[h * NT + d], s.r_hg.at[h * NT + d],
                me, lax.rem(y + d, NT),
            ))
            for d in FAR_T
        ]

    for c in dp_copies:
        c.wait_recv()
    swap = go(remote(s.rows.at[0], s.rows.at[1], s.s_sw.at[0], s.r_sw.at[0], other, y))
    hg_copies = [expert_half(0)]
    swap.wait_recv()
    hg_copies.append(expert_half(1))

    for c in df_copies + dg_copies:
        c.wait_recv()
    group = stacked(s.dg, NZ)
    for k in range(2):
        part = dot_nt(group, s.dw[k]).astype(BF16)
        for t in range(NT):
            s.gp[t, :, k * 512:(k + 1) * 512] = part[t * 16:(t + 1) * 16]
    gr_copies = []
    for d in FAR_T:
        to = lax.rem(y + d, NT)
        gr_copies.append(go(remote(
            s.gp.at[to], s.gr.at[y], s.s_gr.at[d], s.r_gr.at[d], me, to
        )))
    s.gr[y] = s.gp[y]

    rt_copies = []

    def give_back(h):
        for c in hg_copies[h]:
            c.wait_recv()
        acc = dot(s.hg[h, 0], s.ed[0:352])
        for t in range(1, NT):
            acc = acc + dot(s.hg[h, t], s.ed[t * 352:(t + 1) * 352])
        acc = acc.astype(BF16)
        tall = jnp.concatenate([acc[:, t * 128:(t + 1) * 128] for t in range(4)], axis=0)
        back = dot(s.selt[...], tall)
        for i in range(32):
            s.rb[h, i] = back[i * 8:(i + 1) * 8].astype(BF16)
        there = core if h == 0 else 1 - core
        for dx in FAR_X + (0,):
            for dz in FAR_Z + (0,):
                to = lax.rem(z + dz, NZ) * 4 + lax.rem(x + dx, 4)
                k = h * 32 + dz * 4 + dx
                if h or dx or dz:
                    rt_copies.append(go(remote(
                        s.rb.at[h, to], s.ret.at[me], s.s_rt.at[k], s.r_rt.at[k],
                        to * 2 + there, y,
                    )))
                else:
                    s.ret[me] = s.rb[0, chip]

    give_back(0)
    for c in gr_copies:
        c.wait_recv()
    pre = s.gr[0].astype(F32)
    for t in range(1, NT):
        pre = pre + s.gr[t].astype(F32)
    s.dh[y] = (silu(pre[:, :512]) * pre[:, 512:]).astype(BF16)
    dh_copies = [
        go(remote(
            s.dh.at[y], s.dh.at[y], s.s_dh.at[d], s.r_dh.at[d], me, lax.rem(y + d, NT)
        ))
        for d in FAR_T
    ]
    give_back(1)
    for c in dh_copies:
        c.wait_recv()
    part = dot(jnp.concatenate([s.dh[t] for t in range(NT)], axis=0), s.dw[2])
    for i in range(NZ):
        s.op[i] = part[i * 8:(i + 1) * 8].astype(BF16)
    or_copies = []
    for d in FAR_Z:
        to = lax.rem(z + d, NZ)
        or_copies.append(go(remote(
            s.op.at[to], s.orv.at[z], s.s_or.at[d], s.r_or.at[d], to * NQ + q, y
        )))
    s.orv[z] = s.op[z]

    for c in or_copies:
        c.wait_recv()
    dense_out = s.orv[0].astype(F32)
    for i in range(1, NZ):
        dense_out = dense_out + s.orv[i].astype(F32)
    dense_out = dense_out.astype(BF16).astype(F32)
    combined = s.hid[:, pl.ds(pl.multiple_of(y * 512, 512), 512)] + switch * dense_out

    for c in rt_copies:
        c.wait_recv()
    sums = []
    for e in range(16):
        acc = s.ret[4 * e].astype(F32)
        for t in range(1, 4):
            acc = acc + s.ret[4 * e + t].astype(F32)
        sums.append(acc)
    routed = jnp.dot(
        shares, jnp.concatenate(sums, axis=0), preferred_element_type=F32,
        precision=lax.Precision.HIGHEST,
    )
    combined = combined + jnp.concatenate([routed[t * 8:(t + 1) * 8] for t in range(4)], axis=1)
    total = jnp.sum(combined, axis=1, keepdims=True)
    square = jnp.sum(combined * combined, axis=1, keepdims=True)
    s.st[y] = jnp.where(lane < 64, total, square)
    st_copies = [
        go(remote(
            s.st.at[y], s.st.at[y], s.s_st.at[d], s.r_st.at[d], me, lax.rem(y + d, NT)
        ))
        for d in FAR_T
    ]
    for c in sent:
        c.wait_send()
    for c in st_copies:
        c.wait_recv()
    stats = s.st[0] + s.st[1] + s.st[2] + s.st[3]
    mean = stats[:, 0:1] / 2048
    spread = stats[:, 64:65] / 2048 - mean * mean
    result = (combined - mean) * lax.rsqrt(spread + EPS) * s.fin_v[...]
    out[...] = result.astype(BF16)


def body(
    tokens, lengths, cache_keys, cache_values, w_query, w_key, w_value, mix_weight, head_gain,
    w_out, first_gain, routing, route_weights, expert_gate, expert_up, expert_down, dense_gate,
    dense_up, dense_down, switch_vector, final_gain,
):
    hbm = pl.BlockSpec(memory_space=pltpu.HBM)
    return pl.pallas_call(
        layer_kernel,
        out_shape=jax.ShapeDtypeStruct((8, 512), BF16),
        in_specs=[hbm] * 21,
        out_specs=pl.BlockSpec(memory_space=pltpu.VMEM),
        scratch_shapes=list(SCRATCH.values()),
        compiler_params=pltpu.CompilerParams(
            collective_id=0, has_side_effects=True, vmem_limit_bytes=60 * 1024 * 1024
        ),
        name="layer",
    )(
        lengths, mix_weight, routing.T, route_weights.T, tokens,
        cache_keys.reshape(8, 1024, 128), cache_values.reshape(8, 1024, 128),
        w_query, w_key, w_value, w_out.T, head_gain.reshape(1, 128),
        first_gain.reshape(1, 2048), expert_gate[0].T, expert_up[0].T, expert_down[0],
        dense_gate.T, dense_up.T, dense_down, switch_vector.reshape(1, 2048),
        final_gain.reshape(1, 512),
    )


def solution(mesh):
    placed = (
        P("ep", None),
        P("ep"),
        P("ep", "tp", None, None),
        P("ep", "tp", None, None),
        P("ep", "tp"),
        P("ep", "tp"),
        P("ep", "tp"),
        P("tp"),
        P(),
        P("tp", "ep"),
        P(),
        P("ep", None),
        P("ep", None),
        P("ep", None, "tp"),
        P("ep", None, "tp"),
        P("ep", None, "tp"),
        P("tp", "ep"),
        P("tp", "ep"),
        P("ep", "tp"),
        P(),
        P("tp"),
    )
    return jax.shard_map(body, mesh=mesh, in_specs=placed, out_specs=P("ep", "tp"), check_vma=False)
```

```python
from types import SimpleNamespace

import jax
import jax.numpy as jnp
import numpy as np
from jax import lax
from jax.experimental import pallas as pl
from jax.experimental.pallas import tpu as pltpu
from jax.sharding import PartitionSpec as P

EPS = 1e-05

NZ, NQ, NT = 8, 8, 4
FAR_Z = (4, 3, 5, 2, 6, 1, 7)
FAR_Q = (4, 5, 3, 2, 6, 7, 1)
FAR_X = (2, 1, 3)
FAR_T = (2, 1, 3)
MESH_ID = pl.DeviceIdType.MESH
F32 = jnp.float32
ONE = np.ones((2, 8), np.float32)
BF16 = jnp.bfloat16
NT_DIMS = (((1,), (1,)), ((), ()))


def dot(a, b):
    return jnp.dot(a, b, preferred_element_type=F32)


def dot_nt(a, b):
    return lax.dot_general(a, b, NT_DIMS, preferred_element_type=F32)


def stacked(ref, n):
    return jnp.concatenate([ref[i].astype(F32) for i in range(n)], axis=0).astype(BF16)


SCRATCH = dict(
    tok_v=pltpu.VMEM((8, 2048), BF16),
    tokg=pltpu.VMEM((2 * NZ, 8, 256), BF16),
    wmine=pltpu.VMEM((32, 768), BF16),
    wg=pltpu.VMEM((256, 384), BF16),
    wog=pltpu.VMEM((256, 512), BF16),
    kbuf=pltpu.VMEM((8, 1024, 128), BF16),
    vbuf=pltpu.VMEM((8, 1024, 128), BF16),
    fg_v=pltpu.VMEM((1, 2048), F32),
    hg_v=pltpu.VMEM((1, 128), F32),
    sw_v=pltpu.VMEM((1, 2048), F32),
    fin_v=pltpu.VMEM((1, 512), F32),
    pbuf=pltpu.VMEM((2 * NZ, 8, 384), F32),
    precv=pltpu.VMEM((2, NZ, 8, 384), F32),
    qv=pltpu.VMEM((8, 768), F32),
    qs=pltpu.VMEM((8, 8, 128), F32),
    nv=pltpu.VMEM((8, 512), F32),
    ng=pltpu.VMEM((NQ, 8, 512), BF16),
    gbuf=pltpu.VMEM((NQ, 8, 256), BF16),
    attr=pltpu.VMEM((NT, NQ, 8, 256), BF16),
    eg=pltpu.VMEM((352, 2048), BF16),
    eu=pltpu.VMEM((352, 2048), BF16),
    ed=pltpu.VMEM((1408, 512), BF16),
    dw=pltpu.VMEM((3, 512, 512), BF16),
    hid=pltpu.VMEM((8, 2048), F32),
    sel=pltpu.VMEM((128, 128), BF16),
    selt=pltpu.VMEM((128, 128), BF16),
    pk=pltpu.VMEM((16, 8, 512), BF16),
    rows=pltpu.VMEM((4, 16, 8, 512), BF16),
    hg=pltpu.VMEM((4, NT, 32, 352), BF16),
    rb=pltpu.VMEM((4, 16, 8, 128), BF16),
    ret=pltpu.VMEM((64, 8, 128), BF16),
    dg=pltpu.VMEM((NZ, 8, 512), BF16),
    gp=pltpu.VMEM((NT, 16, 1024), BF16),
    gr=pltpu.VMEM((NT, 16, 1024), BF16),
    dh=pltpu.VMEM((NT, 16, 512), BF16),
    op=pltpu.VMEM((NZ, 8, 512), BF16),
    orv=pltpu.VMEM((NZ, 8, 512), BF16),
    st=pltpu.VMEM((NT, 8, 128), F32),
    len_s=pltpu.SMEM((8,), jnp.int32),
    mix_s=pltpu.SMEM((4,), F32),
    rt_s=pltpu.SMEM((2, 8), jnp.int32),
    rw_s=pltpu.SMEM((2, 8), F32),
    lsem=pltpu.SemaphoreType.DMA((21,)),
    s_wg=pltpu.SemaphoreType.DMA((NQ,)),
    r_wg=pltpu.SemaphoreType.DMA((NQ,)),
    s_tok=pltpu.SemaphoreType.DMA((2 * NZ,)),
    r_tok=pltpu.SemaphoreType.DMA((2 * NZ,)),
    s_wo=pltpu.SemaphoreType.DMA((NZ,)),
    r_wo=pltpu.SemaphoreType.DMA((NZ,)),
    s_p=pltpu.SemaphoreType.DMA((2 * NZ,)),
    r_p=pltpu.SemaphoreType.DMA((2 * NZ,)),
    s_n=pltpu.SemaphoreType.DMA((NQ,)),
    r_n=pltpu.SemaphoreType.DMA((NQ,)),
    s_a=pltpu.SemaphoreType.DMA((NT * NQ,)),
    r_a=pltpu.SemaphoreType.DMA((NT * NQ,)),
    s_dw=pltpu.SemaphoreType.DMA((9,)),
    r_dw=pltpu.SemaphoreType.DMA((9,)),
    s_df=pltpu.SemaphoreType.DMA((3,)),
    r_df=pltpu.SemaphoreType.DMA((3,)),
    s_dp=pltpu.SemaphoreType.DMA((2 * NZ,)),
    r_dp=pltpu.SemaphoreType.DMA((2 * NZ,)),
    s_fx=pltpu.SemaphoreType.DMA((2 * NZ,)),
    r_fx=pltpu.SemaphoreType.DMA((2 * NZ,)),
    s_sw=pltpu.SemaphoreType.DMA((2,)),
    r_sw=pltpu.SemaphoreType.DMA((2,)),
    s_dg=pltpu.SemaphoreType.DMA((NZ,)),
    r_dg=pltpu.SemaphoreType.DMA((NZ,)),
    s_gr=pltpu.SemaphoreType.DMA((NT,)),
    r_gr=pltpu.SemaphoreType.DMA((NT,)),
    s_dh=pltpu.SemaphoreType.DMA((NT,)),
    r_dh=pltpu.SemaphoreType.DMA((NT,)),
    s_or=pltpu.SemaphoreType.DMA((NZ,)),
    r_or=pltpu.SemaphoreType.DMA((NZ,)),
    s_hg=pltpu.SemaphoreType.DMA((4 * NT,)),
    r_hg=pltpu.SemaphoreType.DMA((4 * NT,)),
    s_rt=pltpu.SemaphoreType.DMA((64,)),
    r_rt=pltpu.SemaphoreType.DMA((64,)),
    s_st=pltpu.SemaphoreType.DMA((NT,)),
    r_st=pltpu.SemaphoreType.DMA((NT,)),
)


def remote(src, dst, send, recv, ep, tp):
    return pltpu.make_async_remote_copy(
        src_ref=src, dst_ref=dst, send_sem=send, recv_sem=recv,
        device_id=(ep, tp), device_id_type=MESH_ID,
    )


def where_am_i():
    ep, tp = lax.axis_index("ep"), lax.axis_index("tp")
    return ep // NQ, lax.rem(ep, NQ), tp


def placing(e, slot, b, routing, weights):
    rank = jnp.zeros(e.shape, jnp.int32)
    share = jnp.zeros(e.shape, F32)
    for i in range(8):
        first, second = e == routing[0, i], e == routing[1, i]
        rank = rank + jnp.where((first | second) & (b > i), 1, 0)
        mine = jnp.where(first, weights[0, i], jnp.where(second, weights[1, i], 0.0))
        share = jnp.where(b == i, mine, share)
    return jnp.where(rank == slot, share, 0.0)


def silu(v):
    return v / (1.0 + jnp.exp(-v))


def iota2(shape):
    return tuple(lax.broadcasted_iota(jnp.int32, shape, i) for i in range(2))


def layer_kernel(
    lengths, mixw, routing, rweights, tokens, keys, values, wq, wk, wv, wout, hgain, fgain,
    egate, eup, edown, dgate, dup, ddown, switchv, final, out, *scratch
):
    s = SimpleNamespace(**dict(zip(SCRATCH, scratch)))
    z, q, y = where_am_i()
    x, core = q // 2, lax.rem(q, 2)
    me = z * NQ + q
    chip = me // 2
    sent = []

    def go(c):
        c.start()
        sent.append(c)
        return c

    qrow = pl.multiple_of(q * 32, 32)
    zrow = pl.multiple_of(z * 32, 32)
    first = [
        pltpu.make_async_copy(tokens, s.tok_v, s.lsem.at[0]),
        pltpu.make_async_copy(wq, s.wmine.at[:, pl.ds(0, 512)], s.lsem.at[1]),
        pltpu.make_async_copy(wk, s.wmine.at[:, pl.ds(512, 128)], s.lsem.at[2]),
        pltpu.make_async_copy(wv, s.wmine.at[:, pl.ds(640, 128)], s.lsem.at[3]),
        pltpu.make_async_copy(wout, s.wog.at[pl.ds(zrow, 32), :], s.lsem.at[4]),
    ]
    later = [
        pltpu.make_async_copy(keys, s.kbuf, s.lsem.at[5]),
        pltpu.make_async_copy(values, s.vbuf, s.lsem.at[6]),
        pltpu.make_async_copy(fgain, s.fg_v, s.lsem.at[7]),
        pltpu.make_async_copy(hgain, s.hg_v, s.lsem.at[8]),
        pltpu.make_async_copy(lengths, s.len_s, s.lsem.at[17]),
        pltpu.make_async_copy(mixw, s.mix_s, s.lsem.at[18]),
        pltpu.make_async_copy(routing, s.rt_s, s.lsem.at[19]),
        pltpu.make_async_copy(rweights, s.rw_s, s.lsem.at[20]),
    ]
    drow = pl.multiple_of((core * 4 + x) * 64, 64)
    dense = [
        pltpu.make_async_copy(w, s.dw.at[i, pl.ds(drow, 64), :], s.lsem.at[9 + i])
        for i, w in enumerate((dgate, dup, ddown))
    ]
    last = [
        pltpu.make_async_copy(egate, s.eg, s.lsem.at[12]),
        pltpu.make_async_copy(eup, s.eu, s.lsem.at[13]),
        pltpu.make_async_copy(edown, s.ed, s.lsem.at[14]),
        pltpu.make_async_copy(switchv, s.sw_v, s.lsem.at[15]),
        pltpu.make_async_copy(final, s.fin_v, s.lsem.at[16]),
    ]
    for c in first:
        c.start()

    barrier = pltpu.get_barrier_semaphore()
    for d in FAR_Z:
        for swap in range(2):
            to = lax.rem(z + d, NZ) * NQ + x * 2 + lax.rem(core + swap, 2)
            pl.semaphore_signal(barrier, inc=1, device_id=(to, y), device_id_type=MESH_ID)
    for d in FAR_Q:
        pl.semaphore_signal(
            barrier, inc=1, device_id=(z * NQ + lax.rem(q + d, NQ), y), device_id_type=MESH_ID
        )
    for d in FAR_T:
        pl.semaphore_signal(
            barrier, inc=1, device_id=(me, lax.rem(y + d, NT)), device_id_type=MESH_ID
        )
    for c in dense + later:
        c.start()
    i, j = iota2((128, 128))
    s.sel[...] = jnp.where(j == (i % 16) * 8 + (i // 32) * 2 + (i // 16) % 2, 1.0, 0.0).astype(BF16)
    s.selt[...] = jnp.where(i == (j % 16) * 8 + (j // 32) * 2 + (j // 16) % 2, 1.0, 0.0).astype(BF16)
    for c in first:
        c.wait()
    half = pl.ds(pl.multiple_of(core * 384, 384), 384)
    s.wg[pl.ds(qrow, 32), :] = s.wmine[:, half]
    s.tokg[z * 2 + core] = s.tok_v[:, pl.ds(pl.multiple_of(z * 256, 256), 256)]
    pl.semaphore_wait(barrier, 2 * (NZ - 1) + NQ - 1 + NT - 1)

    wg_copies, tok_copies, wo_copies = [], [], []
    for d in FAR_Q:
        to = lax.rem(q + d, NQ)
        theirs = pl.ds(pl.multiple_of(lax.rem(to, 2) * 384, 384), 384)
        wg_copies.append(go(remote(
            s.wmine.at[:, theirs], s.wg.at[pl.ds(qrow, 32), :], s.s_wg.at[d], s.r_wg.at[d],
            z * NQ + to, y,
        )))
    for d in FAR_Z + (0,):
        for swap in range(2):
            if d or swap:
                zz, k = lax.rem(z + d, NZ), d * 2 + swap
                tok_copies.append(go(remote(
                    s.tok_v.at[:, pl.ds(pl.multiple_of(zz * 256, 256), 256)],
                    s.tokg.at[z * 2 + core], s.s_tok.at[k], s.r_tok.at[k],
                    zz * NQ + x * 2 + lax.rem(core + swap, 2), y,
                )))
    for c in last:
        c.start()

    for c in tok_copies + wg_copies:
        c.wait_recv()
    part = dot(stacked(s.tokg, 2 * NZ), s.wg[...])
    for i in range(2 * NZ):
        s.pbuf[i] = part[i * 8:(i + 1) * 8]
    p_copies = []
    for d in FAR_Z + (0,):
        for swap in range(2):
            if d or swap:
                zz, k = lax.rem(z + d, NZ), d * 2 + swap
                cc = lax.rem(core + swap, 2)
                p_copies.append(go(remote(
                    s.pbuf.at[zz * 2 + cc], s.precv.at[core, z], s.s_p.at[k], s.r_p.at[k],
                    zz * NQ + x * 2 + cc, y,
                )))
    for d in FAR_Z:
        mine = s.wog.at[pl.ds(zrow, 32), :]
        wo_copies.append(go(remote(
            mine, mine, s.s_wo.at[d], s.r_wo.at[d], lax.rem(z + d, NZ) * NQ + q, y
        )))
    for c in dense:
        c.wait()
    dw_copies = []
    for i in range(3):
        for d in FAR_X:
            mine = s.dw.at[i, pl.ds(drow, 64), :]
            k = i * 3 + d - 1
            dw_copies.append(go(remote(
                mine, mine, s.s_dw.at[k], s.r_dw.at[k], z * NQ + lax.rem(q + 2 * d, NQ), y
            )))
    s.precv[core, z] = s.pbuf[z * 2 + core]
    for c in p_copies:
        c.wait_recv()
    sides = []
    for h in range(2):
        side = s.precv[h, 0]
        for i in range(1, NZ):
            side = side + s.precv[h, i]
        sides.append(side)
    total = jnp.concatenate(sides, axis=1)
    s.qv[...] = total.astype(BF16).astype(F32)
    for b in range(8):
        for r in range(4):
            row = s.qv[b:b + 1, r * 128:(r + 1) * 128]
            s.qs[b, r:r + 1, :] = row
            s.qs[b, r + 4:r + 5, :] = row

    for c in later:
        c.wait()
    sub = lax.broadcasted_iota(jnp.int32, (8, 128), 0)
    lane = lax.broadcasted_iota(jnp.int32, (8, 128), 1)
    own_half = (sub >= 4) == (lane >= 64)
    col = lax.broadcasted_iota(jnp.int32, (8, 1024), 1)
    rows1 = lax.broadcasted_iota(jnp.int32, (8, 1), 0)
    lam = jnp.zeros((8, 1), F32)
    for r in range(4):
        lam = jnp.where(rows1 == r + 4, s.mix_s[r], lam)
    weight = jnp.where(rows1 < 4, 1.0, -lam)
    empty = jnp.zeros((8, 128), F32)
    for b in range(0, 8, 2):
        pair = (b, b + 1)
        q8 = [jnp.where(own_half, s.qs[i], 0.0) for i in pair]
        wide = jnp.concatenate(
            [jnp.concatenate([q8[0], empty], 1), jnp.concatenate([empty, q8[1]], 1)], 0
        )
        both = jnp.concatenate([s.kbuf[i] for i in pair], axis=1)
        scores = dot_nt(wide.astype(BF16), both) * 0.125
        mixes, owns = [], []
        for k, i in enumerate(pair):
            sc = scores[k * 8:(k + 1) * 8]
            own = jnp.sum(q8[k] * s.qv[i:i + 1, 512:640], axis=1, keepdims=True) * 0.125
            sc = jnp.where(col < s.len_s[i], sc, -jnp.inf)
            top = jnp.maximum(jnp.max(sc, axis=1, keepdims=True), own)
            e = jnp.exp(sc - top)
            eo = jnp.exp(own - top)
            scale = weight / (jnp.sum(e, axis=1, keepdims=True) + eo)
            t = e * scale
            mixes.append(t + pltpu.roll(t, 4, 0))
            to = jnp.broadcast_to(eo * scale, (8, 128))
            mix_own = (to + pltpu.roll(to, 4, 0)).astype(BF16).astype(F32)
            owns.append(mix_own * s.qv[i:i + 1, 640:768])
        both = jnp.concatenate([s.vbuf[i] for i in pair], axis=1)
        heads = dot(jnp.concatenate(mixes, axis=0).astype(BF16), both)
        for k, i in enumerate(pair):
            ho = heads[k * 8:(k + 1) * 8, k * 128:(k + 1) * 128] + owns[k]
            square = jnp.mean(ho * ho, axis=1, keepdims=True)
            n8 = ho * lax.rsqrt(square + EPS) * s.hg_v[...]
            for r in range(4):
                s.nv[i:i + 1, r * 128:(r + 1) * 128] = n8[r:r + 1, :]
    s.ng[q] = s.nv[...].astype(BF16)
    n_copies = []
    for d in FAR_Q:
        c = go(remote(
            s.ng.at[q], s.ng.at[q], s.s_n.at[d], s.r_n.at[d], z * NQ + lax.rem(q + d, NQ), y
        ))
        n_copies.append(c)
    for c in wo_copies + n_copies:
        c.wait_recv()
    group = dot_nt(stacked(s.ng, NQ), s.wog[...])
    for i in range(NQ):
        s.gbuf[i] = group[i * 8:(i + 1) * 8].astype(BF16)
    a_copies = []
    for dq in FAR_Q + (0,):
        for dy in FAR_T + (0,):
            if dy or dq:
                qq = lax.rem(q + dq, NQ)
                c = go(remote(
                    s.gbuf.at[qq], s.attr.at[y, q], s.s_a.at[dy * NQ + dq],
                    s.r_a.at[dy * NQ + dq], z * NQ + qq, lax.rem(y + dy, NT),
                ))
                a_copies.append(c)
    s.attr[y, q] = s.gbuf[q]
    for c in dw_copies:
        c.wait_recv()
    other = me + 1 - 2 * core
    df_copies = []
    for i in range(3):
        mine = s.dw.at[i, pl.ds(pl.multiple_of(core * 256, 256), 256), :]
        df_copies.append(go(remote(mine, mine, s.s_df.at[i], s.r_df.at[i], other, y)))
    for c in a_copies:
        c.wait_recv()
    parts = []
    for i in range(NQ):
        acc = s.attr[0, i].astype(F32)
        for t in range(1, NT):
            acc = acc + s.attr[t, i].astype(F32)
        parts.append(acc)
    lane32 = lane // 32
    tiles = []
    for zz in range(NZ):
        for h in range(2):
            tile = None
            for k in range(4):
                off = zz * 32
                piece = parts[h * 4 + k][:, (off // 128) * 128:(off // 128) * 128 + 128]
                shift = (k * 32 - off % 128) % 128
                if shift:
                    piece = pltpu.roll(piece, shift, 1)
                tile = piece if tile is None else jnp.where(lane32 == k, piece, tile)
            tiles.append(tile)
    state = s.tok_v[...].astype(F32) + jnp.concatenate(tiles, axis=1)
    mean = jnp.mean(state, axis=1, keepdims=True)
    xc = state - mean
    spread = jnp.mean(xc * xc, axis=1, keepdims=True)
    hidden = (xc * lax.rsqrt(spread + EPS) * s.fg_v[...]).astype(BF16)
    hid32 = hidden.astype(F32)
    s.hid[...] = hid32

    s.dg[z] = s.hid[:, pl.ds(pl.multiple_of(y * 512, 512), 512)].astype(BF16)
    dg_copies = [
        go(remote(
            s.dg.at[z], s.dg.at[z], s.s_dg.at[d], s.r_dg.at[d], lax.rem(z + d, NZ) * NQ + q, y
        ))
        for d in FAR_Z
    ]
    i, j = iota2((128, 32))
    ones = placing(i // 8, i % 2, j % 8, s.rt_s, ONE)
    place = jnp.where((i // 2) % 4 == j // 8, ones, 0.0).astype(BF16)
    quarters = jnp.concatenate([hid32[:, t * 512:(t + 1) * 512] for t in range(4)], axis=0)
    packed = dot(place, quarters.astype(BF16))
    for e in range(16):
        s.pk[e] = packed[e * 8:(e + 1) * 8].astype(BF16)
    dp_copies = {}
    for dz in FAR_Z + (0,):
        for side in range(2):
            if dz or side:
                to, k = lax.rem(z + dz, NZ), dz * 2 + side
                tx = 3 - x if side else x
                dp_copies[k] = go(remote(
                    s.pk.at[to * 2 + tx // 2], s.rows.at[0, z * 2 + side], s.s_dp.at[k],
                    s.r_dp.at[k], to * NQ + tx * 2 + core, y,
                ))
    s.rows[0, z * 2] = s.pk[z * 2 + x // 2]
    beside = z * NQ + (x + 1 - 2 * lax.rem(x, 2)) * 2 + core
    fx_copies = []

    def forward(dz, side):
        k = dz * 2 + side
        if k:
            dp_copies[k].wait_recv()
        at = lax.rem(z + NZ - dz, NZ) * 2 + side
        fx_copies.append(go(remote(
            s.rows.at[0, at], s.rows.at[2, at], s.s_fx.at[k], s.r_fx.at[k], beside, y
        )))

    forward(0, 0)
    for c in last:
        c.wait()
    i, j = iota2((32, 128))
    shares = placing(j // 8, j % 2, i % 8, s.rt_s, s.rw_s)
    shares = jnp.where((j // 2) % 4 == i // 8, shares, 0.0)
    switch = 1.0 / (1.0 + jnp.exp(-jnp.sum(hid32 * s.sw_v[...], axis=1, keepdims=True)))

    def expert_part(h):
        block = dot(s.sel[...], jnp.concatenate(
            [s.rows[h, i].astype(F32) for i in range(16)], axis=0).astype(BF16)).astype(BF16)
        wide = jnp.concatenate([block[t * 32:(t + 1) * 32] for t in range(4)], axis=1)
        gate, up = dot_nt(wide, s.eg[...]), dot_nt(wide, s.eu[...])
        s.hg[h, y] = (silu(gate) * up).astype(BF16)
        return [
            go(remote(
                s.hg.at[h, y], s.hg.at[h, y], s.s_hg.at[h * NT + d], s.r_hg.at[h * NT + d],
                me, lax.rem(y + d, NT),
            ))
            for d in FAR_T
        ]

    for dz in FAR_Z[:6]:
        for side in range(2):
            forward(dz, side)
    for c in df_copies + dg_copies:
        c.wait_recv()
    group = stacked(s.dg, NZ)
    for k in range(2):
        part = dot_nt(group, s.dw[k]).astype(BF16)
        for t in range(NT):
            s.gp[t, :, k * 512:(k + 1) * 512] = part[t * 16:(t + 1) * 16]
    gr_copies = []
    for d in FAR_T:
        to = lax.rem(y + d, NT)
        gr_copies.append(go(remote(
            s.gp.at[to], s.gr.at[y], s.s_gr.at[d], s.r_gr.at[d], me, to
        )))
    s.gr[y] = s.gp[y]
    for dz in FAR_Z[6:] + (0,):
        for side in range(2):
            if dz or side:
                forward(dz, side)
    swap0 = go(remote(s.rows.at[0], s.rows.at[1], s.s_sw.at[0], s.r_sw.at[0], other, y))
    hg_copies = [expert_part(0)]
    swap0.wait_recv()
    hg_copies.append(expert_part(1))
    for c in fx_copies:
        c.wait_recv()
    swap1 = go(remote(s.rows.at[2], s.rows.at[3], s.s_sw.at[1], s.r_sw.at[1], other, y))
    hg_copies.append(expert_part(2))
    swap1.wait_recv()
    hg_copies.append(expert_part(3))
    for c in gr_copies:
        c.wait_recv()
    pre = s.gr[0].astype(F32)
    for t in range(1, NT):
        pre = pre + s.gr[t].astype(F32)
    s.dh[y] = (silu(pre[:, :512]) * pre[:, 512:]).astype(BF16)
    dh_copies = [
        go(remote(
            s.dh.at[y], s.dh.at[y], s.s_dh.at[d], s.r_dh.at[d], me, lax.rem(y + d, NT)
        ))
        for d in FAR_T
    ]

    rt_copies = []

    def give_back(h):
        for c in hg_copies[h]:
            c.wait_recv()
        acc = dot(s.hg[h, 0], s.ed[0:352])
        for t in range(1, NT):
            acc = acc + dot(s.hg[h, t], s.ed[t * 352:(t + 1) * 352])
        acc = acc.astype(BF16)
        tall = jnp.concatenate([acc[:, t * 128:(t + 1) * 128] for t in range(4)], axis=0)
        back = dot(s.selt[...], tall)
        for i in range(16):
            s.rb[h, i] = back[i * 8:(i + 1) * 8].astype(BF16)
        there = lax.rem(core + h, 2)
        tx = x + 1 - 2 * lax.rem(x, 2) if h >= 2 else x
        for dz in FAR_Z + (0,):
            for side in range(2):
                to, k = lax.rem(z + dz, NZ), dz * 2 + side
                if h or k:
                    rt_copies.append(go(remote(
                        s.rb.at[h, to * 2 + side], s.ret.at[me], s.s_rt.at[h * 16 + k],
                        s.r_rt.at[h * 16 + k],
                        to * NQ + (3 - tx if side else tx) * 2 + there, y,
                    )))
                else:
                    s.ret[me] = s.rb[0, z * 2]

    give_back(0)
    give_back(1)
    give_back(2)
    give_back(3)
    for c in dh_copies:
        c.wait_recv()
    part = dot(jnp.concatenate([s.dh[t] for t in range(NT)], axis=0), s.dw[2])
    for i in range(NZ):
        s.op[i] = part[i * 8:(i + 1) * 8].astype(BF16)
    or_copies = []
    for d in FAR_Z:
        to = lax.rem(z + d, NZ)
        or_copies.append(go(remote(
            s.op.at[to], s.orv.at[z], s.s_or.at[d], s.r_or.at[d], to * NQ + q, y
        )))
    s.orv[z] = s.op[z]

    for c in or_copies:
        c.wait_recv()
    dense_out = s.orv[0].astype(F32)
    for i in range(1, NZ):
        dense_out = dense_out + s.orv[i].astype(F32)
    dense_out = dense_out.astype(BF16).astype(F32)
    combined = s.hid[:, pl.ds(pl.multiple_of(y * 512, 512), 512)] + switch * dense_out

    for c in rt_copies:
        c.wait_recv()
    sums = []
    for e in range(16):
        acc = s.ret[4 * e].astype(F32)
        for t in range(1, 4):
            acc = acc + s.ret[4 * e + t].astype(F32)
        sums.append(acc)
    routed = jnp.dot(
        shares, jnp.concatenate(sums, axis=0), preferred_element_type=F32,
        precision=lax.Precision.HIGHEST,
    )
    combined = combined + jnp.concatenate([routed[t * 8:(t + 1) * 8] for t in range(4)], axis=1)
    total = jnp.sum(combined, axis=1, keepdims=True)
    square = jnp.sum(combined * combined, axis=1, keepdims=True)
    s.st[y] = jnp.where(lane < 64, total, square)
    st_copies = [
        go(remote(
            s.st.at[y], s.st.at[y], s.s_st.at[d], s.r_st.at[d], me, lax.rem(y + d, NT)
        ))
        for d in FAR_T
    ]
    for c in sent:
        c.wait_send()
    for c in st_copies:
        c.wait_recv()
    stats = s.st[0] + s.st[1] + s.st[2] + s.st[3]
    mean = stats[:, 0:1] / 2048
    spread = stats[:, 64:65] / 2048 - mean * mean
    result = (combined - mean) * lax.rsqrt(spread + EPS) * s.fin_v[...]
    out[...] = result.astype(BF16)


def body(
    tokens, lengths, cache_keys, cache_values, w_query, w_key, w_value, mix_weight, head_gain,
    w_out, first_gain, routing, route_weights, expert_gate, expert_up, expert_down, dense_gate,
    dense_up, dense_down, switch_vector, final_gain,
):
    hbm = pl.BlockSpec(memory_space=pltpu.HBM)
    return pl.pallas_call(
        layer_kernel,
        out_shape=jax.ShapeDtypeStruct((8, 512), BF16),
        in_specs=[hbm] * 21,
        out_specs=pl.BlockSpec(memory_space=pltpu.VMEM),
        scratch_shapes=list(SCRATCH.values()),
        compiler_params=pltpu.CompilerParams(
            collective_id=0, has_side_effects=True, vmem_limit_bytes=60 * 1024 * 1024
        ),
        name="layer",
    )(
        lengths, mix_weight, routing.T, route_weights.T, tokens,
        cache_keys.reshape(8, 1024, 128), cache_values.reshape(8, 1024, 128),
        w_query, w_key, w_value, w_out.T, head_gain.reshape(1, 128),
        first_gain.reshape(1, 2048), expert_gate[0].T, expert_up[0].T, expert_down[0],
        dense_gate.T, dense_up.T, dense_down, switch_vector.reshape(1, 2048),
        final_gain.reshape(1, 512),
    )


def solution(mesh):
    placed = (
        P("ep", None),
        P("ep"),
        P("ep", "tp", None, None),
        P("ep", "tp", None, None),
        P("ep", "tp"),
        P("ep", "tp"),
        P("ep", "tp"),
        P("tp"),
        P(),
        P("tp", "ep"),
        P(),
        P("ep", None),
        P("ep", None),
        P("ep", None, "tp"),
        P("ep", None, "tp"),
        P("ep", None, "tp"),
        P("tp", "ep"),
        P("tp", "ep"),
        P("ep", "tp"),
        P(),
        P("tp"),
    )
    return jax.shard_map(body, mesh=mesh, in_specs=placed, out_specs=P("ep", "tp"), check_vma=False)
```

```python
from types import SimpleNamespace

import jax
import jax.numpy as jnp
import numpy as np
from jax import lax
from jax.experimental import pallas as pl
from jax.experimental.pallas import tpu as pltpu
from jax.sharding import PartitionSpec as P

EPS = 1e-05

NZ, NQ, NT = 8, 8, 4
FAR_Z = (4, 3, 5, 2, 6, 1, 7)
FAR_Q = (4, 5, 3, 2, 6, 7, 1)
FAR_X = (2, 1, 3)
FAR_T = (2, 1, 3)
MESH_ID = pl.DeviceIdType.MESH
F32 = jnp.float32
ONE = np.ones((2, 8), np.float32)
BF16 = jnp.bfloat16
NT_DIMS = (((1,), (1,)), ((), ()))


def dot(a, b):
    return jnp.dot(a, b, preferred_element_type=F32)


def dot_nt(a, b):
    return lax.dot_general(a, b, NT_DIMS, preferred_element_type=F32)


def stacked(ref, n):
    return jnp.concatenate([ref[i].astype(F32) for i in range(n)], axis=0).astype(BF16)


SCRATCH = dict(
    tok_v=pltpu.VMEM((8, 2048), BF16),
    tokg=pltpu.VMEM((2 * NZ, 8, 256), BF16),
    wmine=pltpu.VMEM((32, 768), BF16),
    wg=pltpu.VMEM((256, 384), BF16),
    wog=pltpu.VMEM((256, 512), BF16),
    kbuf=pltpu.VMEM((8, 1024, 128), BF16),
    vbuf=pltpu.VMEM((8, 1024, 128), BF16),
    fg_v=pltpu.VMEM((1, 2048), F32),
    hg_v=pltpu.VMEM((1, 128), F32),
    sw_v=pltpu.VMEM((1, 2048), F32),
    fin_v=pltpu.VMEM((1, 512), F32),
    pbuf=pltpu.VMEM((2 * NZ, 8, 384), F32),
    precv=pltpu.VMEM((2, NZ, 8, 384), F32),
    qv=pltpu.VMEM((8, 768), F32),
    qs=pltpu.VMEM((8, 8, 128), F32),
    nv=pltpu.VMEM((8, 512), F32),
    ng=pltpu.VMEM((NQ, 8, 512), BF16),
    gbuf=pltpu.VMEM((NQ, 8, 256), BF16),
    attr=pltpu.VMEM((NT, NQ, 8, 256), BF16),
    eg=pltpu.VMEM((352, 2048), BF16),
    eu=pltpu.VMEM((352, 2048), BF16),
    ed=pltpu.VMEM((1408, 512), BF16),
    dw=pltpu.VMEM((3, 512, 512), BF16),
    hid=pltpu.VMEM((8, 2048), F32),
    sel=pltpu.VMEM((128, 128), BF16),
    selt=pltpu.VMEM((128, 128), BF16),
    pk=pltpu.VMEM((16, 8, 512), BF16),
    rows=pltpu.VMEM((4, 16, 8, 512), BF16),
    hg=pltpu.VMEM((4, NT, 32, 352), BF16),
    rb=pltpu.VMEM((4, 16, 8, 128), BF16),
    ret=pltpu.VMEM((64, 8, 128), BF16),
    dg=pltpu.VMEM((NZ, 8, 512), BF16),
    gp=pltpu.VMEM((NT, 16, 1024), BF16),
    gr=pltpu.VMEM((NT, 16, 1024), BF16),
    dh=pltpu.VMEM((NT, 16, 512), BF16),
    op=pltpu.VMEM((NZ, 8, 512), BF16),
    orv=pltpu.VMEM((NZ, 8, 512), BF16),
    st=pltpu.VMEM((NT, 8, 128), F32),
    len_s=pltpu.SMEM((8,), jnp.int32),
    mix_s=pltpu.SMEM((4,), F32),
    rt_s=pltpu.SMEM((2, 8), jnp.int32),
    rw_s=pltpu.SMEM((2, 8), F32),
    lsem=pltpu.SemaphoreType.DMA((21,)),
    s_wg=pltpu.SemaphoreType.DMA((NQ,)),
    r_wg=pltpu.SemaphoreType.DMA((NQ,)),
    s_tok=pltpu.SemaphoreType.DMA((2 * NZ,)),
    r_tok=pltpu.SemaphoreType.DMA((2 * NZ,)),
    s_wo=pltpu.SemaphoreType.DMA((NZ,)),
    r_wo=pltpu.SemaphoreType.DMA((NZ,)),
    s_p=pltpu.SemaphoreType.DMA((2 * NZ,)),
    r_p=pltpu.SemaphoreType.DMA((2 * NZ,)),
    s_n=pltpu.SemaphoreType.DMA((NQ,)),
    r_n=pltpu.SemaphoreType.DMA((NQ,)),
    s_a=pltpu.SemaphoreType.DMA((NT * NQ,)),
    r_a=pltpu.SemaphoreType.DMA((NT * NQ,)),
    s_dw=pltpu.SemaphoreType.DMA((9,)),
    r_dw=pltpu.SemaphoreType.DMA((9,)),
    s_df=pltpu.SemaphoreType.DMA((3,)),
    r_df=pltpu.SemaphoreType.DMA((3,)),
    s_dp=pltpu.SemaphoreType.DMA((2 * NZ,)),
    r_dp=pltpu.SemaphoreType.DMA((2 * NZ,)),
    s_fx=pltpu.SemaphoreType.DMA((2 * NZ,)),
    r_fx=pltpu.SemaphoreType.DMA((2 * NZ,)),
    s_sw=pltpu.SemaphoreType.DMA((2,)),
    r_sw=pltpu.SemaphoreType.DMA((2,)),
    s_dg=pltpu.SemaphoreType.DMA((NZ,)),
    r_dg=pltpu.SemaphoreType.DMA((NZ,)),
    s_gr=pltpu.SemaphoreType.DMA((NT,)),
    r_gr=pltpu.SemaphoreType.DMA((NT,)),
    s_dh=pltpu.SemaphoreType.DMA((NT,)),
    r_dh=pltpu.SemaphoreType.DMA((NT,)),
    s_or=pltpu.SemaphoreType.DMA((NZ,)),
    r_or=pltpu.SemaphoreType.DMA((NZ,)),
    s_hg=pltpu.SemaphoreType.DMA((4 * NT,)),
    r_hg=pltpu.SemaphoreType.DMA((4 * NT,)),
    s_rt=pltpu.SemaphoreType.DMA((64,)),
    r_rt=pltpu.SemaphoreType.DMA((64,)),
    s_st=pltpu.SemaphoreType.DMA((NT,)),
    r_st=pltpu.SemaphoreType.DMA((NT,)),
)


def remote(src, dst, send, recv, ep, tp):
    return pltpu.make_async_remote_copy(
        src_ref=src, dst_ref=dst, send_sem=send, recv_sem=recv,
        device_id=(ep, tp), device_id_type=MESH_ID,
    )


def where_am_i():
    ep, tp = lax.axis_index("ep"), lax.axis_index("tp")
    return ep // NQ, lax.rem(ep, NQ), tp


def placing(e, slot, b, routing, weights):
    rank = jnp.zeros(e.shape, jnp.int32)
    share = jnp.zeros(e.shape, F32)
    for i in range(8):
        first, second = e == routing[0, i], e == routing[1, i]
        rank = rank + jnp.where((first | second) & (b > i), 1, 0)
        mine = jnp.where(first, weights[0, i], jnp.where(second, weights[1, i], 0.0))
        share = jnp.where(b == i, mine, share)
    return jnp.where(rank == slot, share, 0.0)


def silu(v):
    return v / (1.0 + jnp.exp(-v))


def iota2(shape):
    return tuple(lax.broadcasted_iota(jnp.int32, shape, i) for i in range(2))


def layer_kernel(
    lengths, mixw, routing, rweights, tokens, keys, values, wq, wk, wv, wout, hgain, fgain,
    egate, eup, edown, dgate, dup, ddown, switchv, final, out, *scratch
):
    s = SimpleNamespace(**dict(zip(SCRATCH, scratch)))
    z, q, y = where_am_i()
    x, core = q // 2, lax.rem(q, 2)
    me = z * NQ + q
    chip = me // 2
    sent = []

    def go(c):
        c.start()
        sent.append(c)
        return c

    qrow = pl.multiple_of(q * 32, 32)
    zrow = pl.multiple_of(z * 32, 32)
    first = [
        pltpu.make_async_copy(tokens, s.tok_v, s.lsem.at[0]),
        pltpu.make_async_copy(wq, s.wmine.at[:, pl.ds(0, 512)], s.lsem.at[1]),
        pltpu.make_async_copy(wk, s.wmine.at[:, pl.ds(512, 128)], s.lsem.at[2]),
        pltpu.make_async_copy(wv, s.wmine.at[:, pl.ds(640, 128)], s.lsem.at[3]),
        pltpu.make_async_copy(wout, s.wog.at[pl.ds(zrow, 32), :], s.lsem.at[4]),
    ]
    later = [
        pltpu.make_async_copy(keys, s.kbuf, s.lsem.at[5]),
        pltpu.make_async_copy(values, s.vbuf, s.lsem.at[6]),
        pltpu.make_async_copy(fgain, s.fg_v, s.lsem.at[7]),
        pltpu.make_async_copy(hgain, s.hg_v, s.lsem.at[8]),
        pltpu.make_async_copy(lengths, s.len_s, s.lsem.at[17]),
        pltpu.make_async_copy(mixw, s.mix_s, s.lsem.at[18]),
        pltpu.make_async_copy(routing, s.rt_s, s.lsem.at[19]),
        pltpu.make_async_copy(rweights, s.rw_s, s.lsem.at[20]),
    ]
    drow = pl.multiple_of((core * 4 + x) * 64, 64)
    dense = [
        pltpu.make_async_copy(w, s.dw.at[i, pl.ds(drow, 64), :], s.lsem.at[9 + i])
        for i, w in enumerate((dgate, dup, ddown))
    ]
    last = [
        pltpu.make_async_copy(egate, s.eg, s.lsem.at[12]),
        pltpu.make_async_copy(eup, s.eu, s.lsem.at[13]),
        pltpu.make_async_copy(edown, s.ed, s.lsem.at[14]),
        pltpu.make_async_copy(switchv, s.sw_v, s.lsem.at[15]),
        pltpu.make_async_copy(final, s.fin_v, s.lsem.at[16]),
    ]
    for c in first:
        c.start()

    barrier = pltpu.get_barrier_semaphore()
    for d in FAR_Z:
        for swap in range(2):
            to = lax.rem(z + d, NZ) * NQ + x * 2 + lax.rem(core + swap, 2)
            pl.semaphore_signal(barrier, inc=1, device_id=(to, y), device_id_type=MESH_ID)
    for d in FAR_Q:
        pl.semaphore_signal(
            barrier, inc=1, device_id=(z * NQ + lax.rem(q + d, NQ), y), device_id_type=MESH_ID
        )
    for d in FAR_T:
        pl.semaphore_signal(
            barrier, inc=1, device_id=(me, lax.rem(y + d, NT)), device_id_type=MESH_ID
        )
    for c in dense + later:
        c.start()
    i, j = iota2((128, 128))
    s.sel[...] = jnp.where(j == (i % 16) * 8 + (i // 32) * 2 + (i // 16) % 2, 1.0, 0.0).astype(BF16)
    s.selt[...] = jnp.where(i == (j % 16) * 8 + (j // 32) * 2 + (j // 16) % 2, 1.0, 0.0).astype(BF16)
    for c in first:
        c.wait()
    half = pl.ds(pl.multiple_of(core * 384, 384), 384)
    s.wg[pl.ds(qrow, 32), :] = s.wmine[:, half]
    s.tokg[z * 2 + core] = s.tok_v[:, pl.ds(pl.multiple_of(z * 256, 256), 256)]
    pl.semaphore_wait(barrier, 2 * (NZ - 1) + NQ - 1 + NT - 1)

    wg_copies, tok_copies, wo_copies = [], [], []
    for d in FAR_Q:
        to = lax.rem(q + d, NQ)
        theirs = pl.ds(pl.multiple_of(lax.rem(to, 2) * 384, 384), 384)
        wg_copies.append(go(remote(
            s.wmine.at[:, theirs], s.wg.at[pl.ds(qrow, 32), :], s.s_wg.at[d], s.r_wg.at[d],
            z * NQ + to, y,
        )))
    for d in FAR_Z + (0,):
        for swap in range(2):
            if d or swap:
                zz, k = lax.rem(z + d, NZ), d * 2 + swap
                tok_copies.append(go(remote(
                    s.tok_v.at[:, pl.ds(pl.multiple_of(zz * 256, 256), 256)],
                    s.tokg.at[z * 2 + core], s.s_tok.at[k], s.r_tok.at[k],
                    zz * NQ + x * 2 + lax.rem(core + swap, 2), y,
                )))
    for c in last:
        c.start()

    for c in tok_copies + wg_copies:
        c.wait_recv()
    part = dot(stacked(s.tokg, 2 * NZ), s.wg[...])
    for i in range(2 * NZ):
        s.pbuf[i] = part[i * 8:(i + 1) * 8]
    p_copies = []
    for d in FAR_Z + (0,):
        for swap in range(2):
            if d or swap:
                zz, k = lax.rem(z + d, NZ), d * 2 + swap
                cc = lax.rem(core + swap, 2)
                p_copies.append(go(remote(
                    s.pbuf.at[zz * 2 + cc], s.precv.at[core, z], s.s_p.at[k], s.r_p.at[k],
                    zz * NQ + x * 2 + cc, y,
                )))
    for d in FAR_Z:
        mine = s.wog.at[pl.ds(zrow, 32), :]
        wo_copies.append(go(remote(
            mine, mine, s.s_wo.at[d], s.r_wo.at[d], lax.rem(z + d, NZ) * NQ + q, y
        )))
    for c in dense:
        c.wait()
    dw_copies = []
    for i in range(3):
        for d in FAR_X:
            mine = s.dw.at[i, pl.ds(drow, 64), :]
            k = i * 3 + d - 1
            dw_copies.append(go(remote(
                mine, mine, s.s_dw.at[k], s.r_dw.at[k], z * NQ + lax.rem(q + 2 * d, NQ), y
            )))
    s.precv[core, z] = s.pbuf[z * 2 + core]
    for c in p_copies:
        c.wait_recv()
    sides = []
    for h in range(2):
        side = s.precv[h, 0]
        for i in range(1, NZ):
            side = side + s.precv[h, i]
        sides.append(side)
    total = jnp.concatenate(sides, axis=1)
    s.qv[...] = total.astype(BF16).astype(F32)
    for b in range(8):
        for r in range(4):
            row = s.qv[b:b + 1, r * 128:(r + 1) * 128]
            s.qs[b, r:r + 1, :] = row
            s.qs[b, r + 4:r + 5, :] = row

    for c in later:
        c.wait()
    sub = lax.broadcasted_iota(jnp.int32, (8, 128), 0)
    lane = lax.broadcasted_iota(jnp.int32, (8, 128), 1)
    own_half = (sub >= 4) == (lane >= 64)
    col = lax.broadcasted_iota(jnp.int32, (8, 1024), 1)
    rows1 = lax.broadcasted_iota(jnp.int32, (8, 1), 0)
    lam = jnp.zeros((8, 1), F32)
    for r in range(4):
        lam = jnp.where(rows1 == r + 4, s.mix_s[r], lam)
    weight = jnp.where(rows1 < 4, 1.0, -lam)
    empty = jnp.zeros((8, 128), F32)
    for b in range(0, 8, 2):
        pair = (b, b + 1)
        q8 = [jnp.where(own_half, s.qs[i], 0.0) for i in pair]
        wide = jnp.concatenate(
            [jnp.concatenate([q8[0], empty], 1), jnp.concatenate([empty, q8[1]], 1)], 0
        )
        both = jnp.concatenate([s.kbuf[i] for i in pair], axis=1)
        scores = dot_nt(wide.astype(BF16), both) * 0.125
        mixes, owns = [], []
        for k, i in enumerate(pair):
            sc = scores[k * 8:(k + 1) * 8]
            own = jnp.sum(q8[k] * s.qv[i:i + 1, 512:640], axis=1, keepdims=True) * 0.125
            sc = jnp.where(col < s.len_s[i], sc, -jnp.inf)
            top = jnp.maximum(jnp.max(sc, axis=1, keepdims=True), own)
            e = jnp.exp(sc - top)
            eo = jnp.exp(own - top)
            scale = weight / (jnp.sum(e, axis=1, keepdims=True) + eo)
            t = e * scale
            mixes.append(t + pltpu.roll(t, 4, 0))
            to = jnp.broadcast_to(eo * scale, (8, 128))
            mix_own = (to + pltpu.roll(to, 4, 0)).astype(BF16).astype(F32)
            owns.append(mix_own * s.qv[i:i + 1, 640:768])
        both = jnp.concatenate([s.vbuf[i] for i in pair], axis=1)
        heads = dot(jnp.concatenate(mixes, axis=0).astype(BF16), both)
        for k, i in enumerate(pair):
            ho = heads[k * 8:(k + 1) * 8, k * 128:(k + 1) * 128] + owns[k]
            square = jnp.mean(ho * ho, axis=1, keepdims=True)
            n8 = ho * lax.rsqrt(square + EPS) * s.hg_v[...]
            for r in range(4):
                s.nv[i:i + 1, r * 128:(r + 1) * 128] = n8[r:r + 1, :]
    s.ng[q] = s.nv[...].astype(BF16)
    n_copies = []
    for d in FAR_Q:
        c = go(remote(
            s.ng.at[q], s.ng.at[q], s.s_n.at[d], s.r_n.at[d], z * NQ + lax.rem(q + d, NQ), y
        ))
        n_copies.append(c)
    for c in wo_copies + n_copies:
        c.wait_recv()
    group = dot_nt(stacked(s.ng, NQ), s.wog[...])
    for i in range(NQ):
        s.gbuf[i] = group[i * 8:(i + 1) * 8].astype(BF16)
    a_copies = []
    for dq in FAR_Q + (0,):
        for dy in FAR_T + (0,):
            if dy or dq:
                qq = lax.rem(q + dq, NQ)
                c = go(remote(
                    s.gbuf.at[qq], s.attr.at[y, q], s.s_a.at[dy * NQ + dq],
                    s.r_a.at[dy * NQ + dq], z * NQ + qq, lax.rem(y + dy, NT),
                ))
                a_copies.append(c)
    s.attr[y, q] = s.gbuf[q]
    for c in dw_copies:
        c.wait_recv()
    other = me + 1 - 2 * core
    df_copies = []
    for i in range(3):
        mine = s.dw.at[i, pl.ds(pl.multiple_of(core * 256, 256), 256), :]
        df_copies.append(go(remote(mine, mine, s.s_df.at[i], s.r_df.at[i], other, y)))
    i, j = iota2((128, 32))
    ones = placing(i // 8, i % 2, j % 8, s.rt_s, ONE)
    place = jnp.where((i // 2) % 4 == j // 8, ones, 0.0).astype(BF16)
    i, j = iota2((32, 128))
    shares = placing(j // 8, j % 2, i % 8, s.rt_s, s.rw_s)
    shares = jnp.where((j // 2) % 4 == i // 8, shares, 0.0)
    for c in a_copies:
        c.wait_recv()
    parts = []
    for i in range(NQ):
        acc = s.attr[0, i].astype(F32)
        for t in range(1, NT):
            acc = acc + s.attr[t, i].astype(F32)
        parts.append(acc)
    lane32 = lane // 32
    tiles = []
    for zz in range(NZ):
        for h in range(2):
            tile = None
            for k in range(4):
                off = zz * 32
                piece = parts[h * 4 + k][:, (off // 128) * 128:(off // 128) * 128 + 128]
                shift = (k * 32 - off % 128) % 128
                if shift:
                    piece = pltpu.roll(piece, shift, 1)
                tile = piece if tile is None else jnp.where(lane32 == k, piece, tile)
            tiles.append(tile)
    state = s.tok_v[...].astype(F32) + jnp.concatenate(tiles, axis=1)
    mean = jnp.mean(state, axis=1, keepdims=True)
    xc = state - mean
    spread = jnp.mean(xc * xc, axis=1, keepdims=True)
    hidden = (xc * lax.rsqrt(spread + EPS) * s.fg_v[...]).astype(BF16)
    hid32 = hidden.astype(F32)
    s.hid[...] = hid32

    s.dg[z] = s.hid[:, pl.ds(pl.multiple_of(y * 512, 512), 512)].astype(BF16)
    dg_copies = [
        go(remote(
            s.dg.at[z], s.dg.at[z], s.s_dg.at[d], s.r_dg.at[d], lax.rem(z + d, NZ) * NQ + q, y
        ))
        for d in FAR_Z
    ]
    quarters = jnp.concatenate([hid32[:, t * 512:(t + 1) * 512] for t in range(4)], axis=0)
    packed = dot(place, quarters.astype(BF16))
    for e in range(16):
        s.pk[e] = packed[e * 8:(e + 1) * 8].astype(BF16)
    dp_copies = {}
    for dz in FAR_Z + (0,):
        for side in range(2):
            if dz or side:
                to, k = lax.rem(z + dz, NZ), dz * 2 + side
                tx = 3 - x if side else x
                dp_copies[k] = go(remote(
                    s.pk.at[to * 2 + tx // 2], s.rows.at[0, z * 2 + side], s.s_dp.at[k],
                    s.r_dp.at[k], to * NQ + tx * 2 + core, y,
                ))
    s.rows[0, z * 2] = s.pk[z * 2 + x // 2]
    beside = z * NQ + (x + 1 - 2 * lax.rem(x, 2)) * 2 + core
    fx_copies = []

    def forward(dz, side):
        k = dz * 2 + side
        if k:
            dp_copies[k].wait_recv()
        at = lax.rem(z + NZ - dz, NZ) * 2 + side
        fx_copies.append(go(remote(
            s.rows.at[0, at], s.rows.at[2, at], s.s_fx.at[k], s.r_fx.at[k], beside, y
        )))

    forward(0, 0)
    for c in last:
        c.wait()
    switch = 1.0 / (1.0 + jnp.exp(-jnp.sum(hid32 * s.sw_v[...], axis=1, keepdims=True)))

    def expert_part(h):
        block = dot(s.sel[...], jnp.concatenate(
            [s.rows[h, i].astype(F32) for i in range(16)], axis=0).astype(BF16)).astype(BF16)
        wide = jnp.concatenate([block[t * 32:(t + 1) * 32] for t in range(4)], axis=1)
        gate, up = dot_nt(wide, s.eg[...]), dot_nt(wide, s.eu[...])
        s.hg[h, y] = (silu(gate) * up).astype(BF16)
        return [
            go(remote(
                s.hg.at[h, y], s.hg.at[h, y], s.s_hg.at[h * NT + d], s.r_hg.at[h * NT + d],
                me, lax.rem(y + d, NT),
            ))
            for d in FAR_T
        ]

    for dz in FAR_Z[:6]:
        for side in range(2):
            forward(dz, side)
    for c in df_copies + dg_copies:
        c.wait_recv()
    group = stacked(s.dg, NZ)
    for k in range(2):
        part = dot_nt(group, s.dw[k]).astype(BF16)
        for t in range(NT):
            s.gp[t, :, k * 512:(k + 1) * 512] = part[t * 16:(t + 1) * 16]
    gr_copies = []
    for d in FAR_T:
        to = lax.rem(y + d, NT)
        gr_copies.append(go(remote(
            s.gp.at[to], s.gr.at[y], s.s_gr.at[d], s.r_gr.at[d], me, to
        )))
    s.gr[y] = s.gp[y]
    for dz in FAR_Z[6:] + (0,):
        for side in range(2):
            if dz or side:
                forward(dz, side)
    swap0 = go(remote(s.rows.at[0], s.rows.at[1], s.s_sw.at[0], s.r_sw.at[0], other, y))
    hg_copies = [expert_part(0)]
    swap0.wait_recv()
    hg_copies.append(expert_part(1))
    for c in fx_copies:
        c.wait_recv()
    swap1 = go(remote(s.rows.at[2], s.rows.at[3], s.s_sw.at[1], s.r_sw.at[1], other, y))
    hg_copies.append(expert_part(2))
    swap1.wait_recv()
    hg_copies.append(expert_part(3))
    for c in gr_copies:
        c.wait_recv()
    pre = s.gr[0].astype(F32)
    for t in range(1, NT):
        pre = pre + s.gr[t].astype(F32)
    s.dh[y] = (silu(pre[:, :512]) * pre[:, 512:]).astype(BF16)
    dh_copies = [
        go(remote(
            s.dh.at[y], s.dh.at[y], s.s_dh.at[d], s.r_dh.at[d], me, lax.rem(y + d, NT)
        ))
        for d in FAR_T
    ]

    rt_copies = []

    def give_back(h):
        for c in hg_copies[h]:
            c.wait_recv()
        acc = dot(s.hg[h, 0], s.ed[0:352])
        for t in range(1, NT):
            acc = acc + dot(s.hg[h, t], s.ed[t * 352:(t + 1) * 352])
        acc = acc.astype(BF16)
        tall = jnp.concatenate([acc[:, t * 128:(t + 1) * 128] for t in range(4)], axis=0)
        back = dot(s.selt[...], tall)
        for i in range(16):
            s.rb[h, i] = back[i * 8:(i + 1) * 8].astype(BF16)
        there = lax.rem(core + h, 2)
        tx = x + 1 - 2 * lax.rem(x, 2) if h >= 2 else x
        for dz in FAR_Z + (0,):
            for side in range(2):
                to, k = lax.rem(z + dz, NZ), dz * 2 + side
                if h or k:
                    rt_copies.append(go(remote(
                        s.rb.at[h, to * 2 + side], s.ret.at[me], s.s_rt.at[h * 16 + k],
                        s.r_rt.at[h * 16 + k],
                        to * NQ + (3 - tx if side else tx) * 2 + there, y,
                    )))
                else:
                    s.ret[me] = s.rb[0, z * 2]

    give_back(0)
    give_back(1)
    give_back(2)
    give_back(3)
    for c in dh_copies:
        c.wait_recv()
    part = dot(jnp.concatenate([s.dh[t] for t in range(NT)], axis=0), s.dw[2])
    for i in range(NZ):
        s.op[i] = part[i * 8:(i + 1) * 8].astype(BF16)
    or_copies = []
    for d in FAR_Z:
        to = lax.rem(z + d, NZ)
        or_copies.append(go(remote(
            s.op.at[to], s.orv.at[z], s.s_or.at[d], s.r_or.at[d], to * NQ + q, y
        )))
    s.orv[z] = s.op[z]

    for c in or_copies:
        c.wait_recv()
    dense_out = s.orv[0].astype(F32)
    for i in range(1, NZ):
        dense_out = dense_out + s.orv[i].astype(F32)
    dense_out = dense_out.astype(BF16).astype(F32)
    combined = s.hid[:, pl.ds(pl.multiple_of(y * 512, 512), 512)] + switch * dense_out

    for c in rt_copies:
        c.wait_recv()
    sums = []
    for e in range(16):
        acc = s.ret[4 * e].astype(F32)
        for t in range(1, 4):
            acc = acc + s.ret[4 * e + t].astype(F32)
        sums.append(acc)
    routed = jnp.dot(
        shares, jnp.concatenate(sums, axis=0), preferred_element_type=F32,
        precision=lax.Precision.HIGHEST,
    )
    combined = combined + jnp.concatenate([routed[t * 8:(t + 1) * 8] for t in range(4)], axis=1)
    total = jnp.sum(combined, axis=1, keepdims=True)
    square = jnp.sum(combined * combined, axis=1, keepdims=True)
    s.st[y] = jnp.where(lane < 64, total, square)
    st_copies = [
        go(remote(
            s.st.at[y], s.st.at[y], s.s_st.at[d], s.r_st.at[d], me, lax.rem(y + d, NT)
        ))
        for d in FAR_T
    ]
    for c in sent:
        c.wait_send()
    for c in st_copies:
        c.wait_recv()
    stats = s.st[0] + s.st[1] + s.st[2] + s.st[3]
    mean = stats[:, 0:1] / 2048
    spread = stats[:, 64:65] / 2048 - mean * mean
    result = (combined - mean) * lax.rsqrt(spread + EPS) * s.fin_v[...]
    out[...] = result.astype(BF16)


def body(
    tokens, lengths, cache_keys, cache_values, w_query, w_key, w_value, mix_weight, head_gain,
    w_out, first_gain, routing, route_weights, expert_gate, expert_up, expert_down, dense_gate,
    dense_up, dense_down, switch_vector, final_gain,
):
    hbm = pl.BlockSpec(memory_space=pltpu.HBM)
    return pl.pallas_call(
        layer_kernel,
        out_shape=pltpu.VMEM((8, 512), BF16),
        in_specs=[hbm] * 21,
        out_specs=pl.BlockSpec(memory_space=pltpu.VMEM),
        scratch_shapes=list(SCRATCH.values()),
        compiler_params=pltpu.CompilerParams(
            collective_id=0, has_side_effects=True, vmem_limit_bytes=60 * 1024 * 1024
        ),
        name="layer",
    )(
        lengths, mix_weight, routing.T, route_weights.T, tokens,
        cache_keys.reshape(8, 1024, 128), cache_values.reshape(8, 1024, 128),
        w_query, w_key, w_value, w_out.T, head_gain.reshape(1, 128),
        first_gain.reshape(1, 2048), expert_gate[0].T, expert_up[0].T, expert_down[0],
        dense_gate.T, dense_up.T, dense_down, switch_vector.reshape(1, 2048),
        final_gain.reshape(1, 512),
    )


def solution(mesh):
    placed = (
        P("ep", None),
        P("ep"),
        P("ep", "tp", None, None),
        P("ep", "tp", None, None),
        P("ep", "tp"),
        P("ep", "tp"),
        P("ep", "tp"),
        P("tp"),
        P(),
        P("tp", "ep"),
        P(),
        P("ep", None),
        P("ep", None),
        P("ep", None, "tp"),
        P("ep", None, "tp"),
        P("ep", None, "tp"),
        P("tp", "ep"),
        P("tp", "ep"),
        P("ep", "tp"),
        P(),
        P("tp"),
    )
    return jax.shard_map(body, mesh=mesh, in_specs=placed, out_specs=P("ep", "tp"), check_vma=False)
```
